256 devices in a mesh: grp: 2 (over z), ep: 16 (over y, core), tp: 8 (over x).
Axes of the slice: x: 8, y: 8, z: 2, core: 2. Of those that a mesh axis runs over, the one named last changes fastest.
The devices are a block of a 8x8x16 slice.
Arguments:
- tokens: bfloat16 [8192, 4096], P(('grp', 'ep')), parts along dimension 0, may hold values from -6 to 6
- expert_ids: int32 [8192, 2], P(('grp', 'ep')), parts along dimension 0, may hold values from 0 to 15, as said below
- gates: float32 [8192, 2], P(('grp', 'ep')), parts along dimension 0, may hold values from 0.1 to 1
- w_gate: bfloat16 [16, 4096, 2048], P('ep', None, 'tp'), may hold values from -0.09375 to 0.09375
- w_up: bfloat16 [16, 4096, 2048], P('ep', None, 'tp'), may hold values from -0.09375 to 0.09375
- w_down: bfloat16 [16, 2048, 4096], P('ep', 'tp'), may hold values from -0.79549513 to 0.79549513, as said below
- norm_gain: float32 [4096], P('tp'), may hold values from 0.1 to 1.9
- norm_bias: float32 [4096], P('tp'), may hold values from -1.5 to 1.5
Outputs:
- normed: bfloat16 [8192, 4096], P(('grp', 'ep'), 'tp'), parts along dimension 0
The draws below stay inside these ranges and needn't reach their ends.
There are 2 independent parts, one for each index of `grp`. The reference program is written for one: setup_inputs(seed, part) draws one part's arguments, and reference() takes and returns one part's arrays. A program takes and returns all parts, laid end to end along the dimension named above; an argument that names none is the same for every part. Nothing has to cross between parts.
Inputs may be any that keep to these rules, and one draw needn't show every extreme that they name: `expert_ids`: each row names 2 different experts, both in the same group of 4 consecutive expert numbers. Within one aligned block of 256 rows no expert is named more than 64 times, and in every draw some expert is named exactly 64 times in every block. `w_down`: down projection weights.
All inputs are finite; a program needn't handle non-finite values.
Results may differ from the reference program's by a relative error of at most 0.014.
Values may be sent and summed in bfloat16 or wider, within the bound.
A program may use at most 128 MiB of HBM per device.

```python
import math
import jax
import jax.numpy as jnp
from jax import lax

D = 4096
FF = 2048
GROUPS = 4
EXPERTS_PER_GROUP = 4
TOPK = 2
TOK_DEV = 256
EXPERTS = 16
CAP = 64
SLOTS = 1024
FF_DEV = 256
TOKENS = 4096
N_EP = 16
N_TP = 8


def route_block(block_key, busy_group):
    key_weights, key_labels, key_shuffle = jax.random.split(block_key, 3)
    weights = jax.random.randint(key_weights, (GROUPS,), 4, 9)
    is_busy = jnp.arange(GROUPS) == busy_group
    weights = jnp.where(is_busy, 0, weights)
    busy_count = TOK_DEV // 2
    remainder = TOK_DEV - busy_count
    counts = remainder * weights // jnp.sum(weights)
    leftover = remainder - jnp.sum(counts)
    first_other = jnp.argmin(is_busy.astype(jnp.int32))
    counts = counts + leftover * (jnp.arange(GROUPS) == first_other).astype(jnp.int32)
    counts = jnp.where(is_busy, busy_count, counts)
    group_ends = jnp.cumsum(counts)
    group_starts = group_ends - counts
    position = jnp.arange(TOK_DEV)
    group_of = jnp.sum((position[:, None] >= group_ends[None, :]).astype(jnp.int32), axis=1)
    within = position - group_starts[group_of]
    first_table = jnp.array([0, 2, 0, 1, 0, 1], jnp.int32)
    second_table = jnp.array([1, 3, 2, 3, 3, 2], jnp.int32)
    relabel = jax.vmap(lambda label_key: jax.random.permutation(label_key, EXPERTS_PER_GROUP))(jax.random.split(key_labels, GROUPS))
    group_base = group_of * EXPERTS_PER_GROUP
    first_expert = group_base + relabel[group_of, first_table[within % 6]]
    second_expert = group_base + relabel[group_of, second_table[within % 6]]
    chosen = jnp.stack([first_expert, second_expert], axis=1).astype(jnp.int32)
    shuffle = jax.random.permutation(key_shuffle, TOK_DEV)
    return chosen[shuffle]


def draw_expert_ids(key, part):
    busy_group = jax.random.randint(jax.random.fold_in(key, 7), (), 0, GROUPS)
    block_keys = jax.random.split(jax.random.fold_in(key, 11), TOKENS // TOK_DEV)
    chosen = jax.vmap(route_block, in_axes=(0, None))(block_keys, busy_group)
    return chosen.reshape(TOKENS, TOPK).astype(jnp.int32)


def draw_w_down(key, part):
    noise = jnp.clip(jax.random.normal(jax.random.fold_in(key, 3), (EXPERTS, FF, D), jnp.float32), -6.0, 6.0)
    columns = 0.6 * jnp.exp(math.log(3.0) * jnp.arange(D, dtype=jnp.float32) / (D - 1))
    return (noise * FF ** (-0.5) * columns).astype(jnp.bfloat16)


def shard_levels(key, extent, shards, low, top_value):
    gain = 1.0
    for dim, shards_of in shards:
        draws = jax.random.uniform(jax.random.fold_in(jax.random.fold_in(key, 6), dim), (shards_of,), jnp.float32, low / len(shards), top_value / len(shards))
        gain = gain * jnp.repeat(jnp.exp(draws), extent[dim] // shards_of).reshape((-1,) + (1,) * (len(extent) - 1 - dim))
    return gain


def normal_values(key, shape, width, limit, cuts=(), kind=jnp.bfloat16):
    drawn = width * jax.random.normal(key, shape, jnp.float32)
    if cuts:
        drawn = drawn * shard_levels(key, shape, cuts, -0.22, 0.18)
    return jnp.clip(drawn, -limit, limit).astype(kind)


def setup_inputs(seed: int = 0, part: int = 0) -> dict:
    seeds = jax.random.split(jax.random.key(seed), 9)
    part_splits = jax.random.split(jax.random.fold_in(seeds[8], part), 9)
    tokens = normal_values(part_splits[0], (TOKENS, D), 1.0, 6.0, ((0, 16),))
    expert_ids = draw_expert_ids(jax.random.fold_in(jax.random.fold_in(seeds[8], part), 71), part)
    gates = jnp.clip(0.1 + 0.9 * jax.random.uniform(part_splits[2], (TOKENS, TOPK), jnp.float32) ** shard_levels(part_splits[2], (TOKENS, TOPK), ((0, 16),), -0.2, 0.2), 0.1, 1.0)
    w_gate = normal_values(seeds[3], (EXPERTS, D, FF), D ** -0.5, 0.09375, ((0, 16), (2, 8)))
    w_up = normal_values(seeds[4], (EXPERTS, D, FF), D ** -0.5, 0.09375, ((0, 16), (2, 8)))
    w_down = draw_w_down(jax.random.fold_in(seeds[8], 71), part)
    norm_gain = jnp.clip(1.0 + 0.18 * jax.random.normal(seeds[6], (D,), jnp.float32), 0.1, 1.9)
    norm_bias = normal_values(seeds[7], (D,), 0.3, 1.5, ((0, 8),), jnp.float32)
    return dict(tokens=tokens, expert_ids=expert_ids, gates=gates, w_gate=w_gate, w_up=w_up, w_down=w_down, norm_gain=norm_gain, norm_bias=norm_bias)


norm_eps = 1e-05

def run_expert(operands):
    routed, gate_w, up_w, down_w = operands
    gate_part = jnp.dot(routed, gate_w, preferred_element_type=jnp.float32)
    up_part = jnp.dot(routed, up_w, preferred_element_type=jnp.float32)
    hidden = (jax.nn.silu(gate_part) * up_part).astype(jnp.bfloat16)
    blocks = hidden.reshape(SLOTS, N_TP, FF_DEV).astype(jnp.float32)
    down_blocks = down_w.reshape(N_TP, FF_DEV, D).astype(jnp.float32)
    partial_value = jnp.einsum('rjf,jfd->jrd', blocks, down_blocks).astype(jnp.bfloat16)
    partial_value = lax.optimization_barrier(partial_value)
    return lax.optimization_barrier(jnp.sum(partial_value.astype(jnp.float32), axis=0)).astype(jnp.bfloat16)

def reference(tokens, expert_ids, gates, w_gate, w_up, w_down, norm_gain, norm_bias):
    flat_ids = expert_ids.reshape(N_EP, TOK_DEV * TOPK)
    onehot = (flat_ids[:, :, None] == jnp.arange(EXPERTS, dtype=jnp.int32)[None, None, :]).astype(jnp.int32)
    position = lax.optimization_barrier(jnp.sum((jnp.cumsum(onehot, axis=1) - 1) * onehot, axis=2))
    source_block = jnp.arange(N_EP, dtype=jnp.int32)[:, None]
    target = (flat_ids * SLOTS + source_block * CAP + position).reshape(-1).astype(jnp.int32)
    token_of = jnp.arange(TOKENS * TOPK, dtype=jnp.int32) // TOPK
    source = jnp.zeros((EXPERTS * SLOTS,), jnp.int32).at[target].set(token_of)
    filled = jnp.zeros((EXPERTS * SLOTS,), jnp.bool_).at[target].set(True)
    routed = jnp.where(filled[:, None], tokens[source], jnp.zeros((), jnp.bfloat16)).reshape(EXPERTS, SLOTS, D)
    expert_out = lax.map(run_expert, (routed, w_gate, w_up, w_down))
    picked = expert_out.reshape(EXPERTS * SLOTS, D)[target].reshape(TOKENS, TOPK, D)
    combined = lax.optimization_barrier(jnp.sum(picked.astype(jnp.float32) * gates[:, :, None], axis=1))
    row_mean = lax.optimization_barrier(jnp.mean(combined, axis=1, keepdims=True))
    centred = combined - row_mean
    row_var = lax.optimization_barrier(jnp.mean(centred * centred, axis=1, keepdims=True))
    normed = centred * lax.rsqrt(row_var + norm_eps) * norm_gain + norm_bias
    return normed.astype(jnp.bfloat16)
```

```python
import functools

import jax
import jax.numpy as jnp
from jax import lax
from jax.experimental import pallas as pl
from jax.experimental.pallas import tpu as pltpu
from jax.sharding import PartitionSpec as P

CAP = 64
CORES = 2
EPS = 1e-05
BF = jnp.bfloat16
F32 = jnp.float32


def dot(a, b):
    return jnp.dot(a, b, preferred_element_type=F32)


def offset_of(i):
    half = (i + 1) // 2
    return half * (2 * lax.rem(i, 2) - 1)


def kernel(
    n_ep, n_tp, n_grp,
    tok_hbm, ids_ref, gates_ref, wg_hbm, wu_hbm, wd_hbm, gain_ref, bias_ref,
    out_ref,
    tok, wg, wu, wdc, routed, sendb, sib, hid, outb, ret, slots, stat,
    load_sem,
    ys_sem, yr_sem, xs_sem, xr_sem, hs_sem, hr_sem, rs_sem, rr_sem,
    ws_sem, wr_sem, zs_sem, zr_sem, ss_sem, sr_sem,
):
    n_y = n_ep // CORES
    tokens, width = tok.shape
    quarter = width // 4
    cols = width // n_tp
    ff = wg.shape[1]
    rows = CORES * CAP
    far = n_tp // 2
    me_g, me_e, me_x = (lax.axis_index(a) for a in ("grp", "ep", "tp"))
    me_y, me_c = me_e // CORES, lax.rem(me_e, CORES)
    half = lax.rem(me_x, 2)
    right, left = lax.rem(me_x + 1, n_tp), lax.rem(me_x + n_tp - 1, n_tp)
    mate = me_g + 1 - 2 * lax.rem(me_g, 2)
    wpart = lax.rem(me_g, 2)

    def x_at(s):
        return lax.rem(me_x + s + n_tp, n_tp)

    def chip_at(i):
        return lax.rem(me_y + offset_of(i) + n_y, n_y)

    def chunk_rows(chip):
        return pl.ds(pl.multiple_of(chip * rows, rows), rows)

    def block_rows(block):
        return pl.ds(pl.multiple_of(block * CAP, CAP), CAP)

    load_tok = pltpu.make_async_copy(tok_hbm, tok, load_sem.at[0])
    load_wg = pltpu.make_async_copy(wg_hbm, wg, load_sem.at[1])
    load_wu = pltpu.make_async_copy(wu_hbm, wu, load_sem.at[2])
    own_cols = pl.ds(pl.multiple_of(me_x * cols, cols), cols)
    own_w = pl.ds(pl.multiple_of(me_x * ff, ff), ff)
    load_wd = pltpu.make_async_copy(wd_hbm.at[:, own_cols], wdc.at[own_w], load_sem.at[3])
    load_tok.start()
    load_wg.start()
    load_wu.start()
    load_wd.start()

    barrier = pltpu.get_barrier_semaphore()
    for s in range(1, n_ep):
        pl.semaphore_signal(barrier, 1, device_id={"ep": lax.rem(me_e + s, n_ep)})
    for s in range(1, n_tp):
        pl.semaphore_signal(barrier, 1, device_id={"tp": lax.rem(me_x + s, n_tp)})
    pl.semaphore_signal(barrier, 1, device_id={"grp": mate})

    ids = ids_ref[...]
    lane = lax.broadcasted_iota(jnp.int32, (tokens, 128), 1)
    hit0 = lane == ids[:, 0:1]
    hit1 = lane == ids[:, 1:2]
    named = jnp.where(hit0 | hit1, 1.0, 0.0).astype(BF)
    t_row = lax.broadcasted_iota(jnp.int32, (tokens, tokens), 0)
    t_col = lax.broadcasted_iota(jnp.int32, (tokens, tokens), 1)
    before = jnp.where(t_col < t_row, 1.0, 0.0).astype(BF)
    position = dot(before, named)
    slot = position + (lane * CAP).astype(F32)
    slot0 = jnp.sum(jnp.where(hit0, slot, 0.0), axis=1, keepdims=True)
    slot1 = jnp.sum(jnp.where(hit1, slot, 0.0), axis=1, keepdims=True)
    slots[...] = jnp.where(lane == 0, slot0, jnp.where(lane == 1, slot1, -1.0)).T[:8]

    pl.semaphore_wait(barrier, n_ep - 1 + n_tp - 1 + 1)

    wrows = ff // 2

    def w_half(x, part):
        return pl.ds(pl.multiple_of(x * ff + part * wrows, wrows), wrows)

    def w_copy(i):
        x = x_at(offset_of(i + 1))
        return pltpu.make_async_remote_copy(
            wd_hbm.at[
                pl.ds(pl.multiple_of(wpart * wrows, wrows), wrows),
                pl.ds(pl.multiple_of(x * cols, cols), cols),
            ],
            wdc.at[w_half(me_x, wpart)],
            ws_sem.at[x], wr_sem.at[me_x], device_id={"tp": x},
        )

    def w_arrival(x):
        here = wdc.at[w_half(x, wpart)]
        return pltpu.make_async_remote_copy(
            here, here, ws_sem.at[x], wr_sem.at[x], device_id={"tp": x})

    def z_copy(x, part):
        here = wdc.at[w_half(x, part)]
        return pltpu.make_async_remote_copy(
            here, here, zs_sem.at[x], zr_sem.at[x], device_id={"grp": mate})

    @pl.loop(0, n_tp - 1)
    def _(i):
        w_copy(i).start()

    load_tok.wait()

    def spread(chip, column):
        s_iota = (chip * rows).astype(F32) + lax.broadcasted_iota(
            jnp.int32, (rows, tokens), 0).astype(F32)
        chosen = (s_iota == slots[0:1, :]) | (s_iota == slots[1:2, :])
        pick = jnp.where(chosen, 1.0, 0.0).astype(BF)
        return dot(pick, tok[:, pl.ds(pl.multiple_of(column, quarter), quarter)]).astype(BF)

    def y_copy(chip, core):
        expert = chip * CORES + core
        return pltpu.make_async_remote_copy(
            sendb.at[:, block_rows(expert)],
            routed.at[pl.ds(2 * half, 2), block_rows(me_e)],
            ys_sem.at[expert], yr_sem.at[me_e], device_id={"ep": expert},
        )

    def y_arrival(block):
        here = routed.at[pl.ds(2 * half, 2), block_rows(block)]
        return pltpu.make_async_remote_copy(
            here, here, ys_sem.at[block], yr_sem.at[block], device_id={"ep": block})

    sibling = me_y * CORES + 1 - me_c

    def sib_copy():
        return pltpu.make_async_remote_copy(
            sib, routed.at[:, block_rows(me_e)],
            ys_sem.at[sibling], yr_sem.at[me_e], device_id={"ep": sibling},
        )

    def sib_arrival():
        here = routed.at[:, block_rows(sibling)]
        return pltpu.make_async_remote_copy(
            here, here, ys_sem.at[sibling], yr_sem.at[sibling], device_id={"ep": sibling})

    @pl.loop(1, n_y)
    def _(i):
        chip = chip_at(i)
        for q in range(2):
            sendb[q, chunk_rows(chip), :] = spread(chip, (2 * half + q) * quarter)
        for core in range(CORES):
            y_copy(chip, core).start()

    @pl.loop(0, 4)
    def _(q):
        both = spread(me_y, q * quarter)
        swap = me_c == 0
        routed[q, block_rows(me_e), :] = jnp.where(swap, both[:CAP], both[CAP:])
        sib[q] = jnp.where(swap, both[CAP:], both[:CAP])

    sib_copy().start()

    def x_copy(chip, side):
        here = routed.at[2 * half + side, chunk_rows(chip)]
        return pltpu.make_async_remote_copy(
            here, here, xs_sem.at[side, chip], xr_sem.at[side, chip],
            device_id={"tp": (right, left)[side]})

    def x_arrival(chip, side):
        here = routed.at[2 * (1 - half) + side, chunk_rows(chip)]
        return pltpu.make_async_remote_copy(
            here, here, xs_sem.at[side, chip], xr_sem.at[side, chip],
            device_id={"tp": (left, right)[side]})

    def hid_part(chip, x, step, side):
        if step < far:
            return hid.at[x, chunk_rows(chip)]
        first = pl.multiple_of(chip * rows + side * CAP, CAP)
        return hid.at[x, pl.ds(first, rows // 2)]

    def hid_copy(chip, step, side):
        x = x_at((1 - step, step - 1)[side])
        here = hid_part(chip, x, step, side)
        return pltpu.make_async_remote_copy(
            here, here, hs_sem.at[side, step - 1, chip], hr_sem.at[side, step - 1, chip],
            device_id={"tp": (right, left)[side]})

    def hid_arrival(chip, step, side):
        x = x_at((-step, step)[side])
        here = hid_part(chip, x, step, side)
        return pltpu.make_async_remote_copy(
            here, here, hs_sem.at[side, step - 1, chip], hr_sem.at[side, step - 1, chip],
            device_id={"tp": (left, right)[side]})

    def ret_copy(chip, core):
        block = chip * CORES + core
        return pltpu.make_async_remote_copy(
            outb.at[block_rows(block)], ret.at[block_rows(me_e)],
            rs_sem.at[block], rr_sem.at[me_e], device_id={"ep": block})

    def ret_arrival(expert):
        here = ret.at[block_rows(expert)]
        return pltpu.make_async_remote_copy(
            here, here, rs_sem.at[expert], rr_sem.at[expert], device_id={"ep": expert})

    def forward(chip):
        for core in range(CORES):
            y_arrival(chip * CORES + core).wait_recv()
        for side in range(2):
            x_copy(chip, side).start()

    def first_layers(chip):
        here = chunk_rows(chip)
        gate = jnp.zeros((rows, ff), F32)
        up = jnp.zeros((rows, ff), F32)
        for q in range(4):
            part = routed[q, here, :]
            at = slice(q * quarter, (q + 1) * quarter)
            gate += dot(part, wg[at, :])
            up += dot(part, wu[at, :])
        hid[me_x, here, :] = (gate / (1.0 + jnp.exp(-gate)) * up).astype(BF)
        for side in range(2):
            hid_copy(chip, 1, side).start()

    def relay(chip, step):
        for side in range(2):
            hid_arrival(chip, step, side).wait_recv()
            hid_copy(chip, step + 1, side).start()

    def last_layer(chip):
        for side in range(2):
            hid_arrival(chip, far, side).wait_recv()
        here = chunk_rows(chip)
        acc = jnp.zeros((rows, cols), F32)
        for j in range(n_tp):
            acc += dot(hid[j, here, :], wdc[j * ff:(j + 1) * ff, :])
        outb[here, :] = acc.astype(BF)

    stages = far + 2
    lag_last = stages - 1

    @pl.loop(0, n_y + lag_last)
    def _(t):
        c = t - lag_last

        @pl.when(c == 0)
        def _():
            @pl.loop(1, n_tp)
            def _(s):
                z_copy(x_at(s), 1 - wpart).wait_recv()
            load_wd.wait()

        @pl.when((c >= 0) & (c < n_y))
        def _():
            chip = chip_at(c)
            last_layer(chip)

            @pl.when(c == 0)
            def _():
                ret[block_rows(me_e), :] = outb[block_rows(me_e), :]
                ret_copy(me_y, 1 - me_c).start()

            @pl.when(c > 0)
            def _():
                for core in range(CORES):
                    ret_copy(chip, core).start()

        for step in range(far - 1, 0, -1):
            r = t - 1 - step

            @pl.when((r >= 0) & (r < n_y))
            def _():
                relay(chip_at(r), step)

        b = t - 1

        @pl.when(b == 0)
        def _():
            sib_arrival().wait_recv()
            load_wg.wait()
            load_wu.wait()

        @pl.when((b >= 0) & (b < n_y))
        def _():
            chip = chip_at(b)

            @pl.when(b > 0)
            def _():
                for side in range(2):
                    x_arrival(chip, side).wait_recv()

            first_layers(chip)

        @pl.when((t > 0) & (t < n_y))
        def _():
            forward(chip_at(t))

        @pl.when(t == 3)
        def _():
            @pl.loop(1, n_tp)
            def _(s):
                x = x_at(s)
                w_arrival(x).wait_recv()
                z_copy(x, wpart).start()

    s_iota = lax.broadcasted_iota(jnp.int32, (tokens, n_ep * CAP), 1).astype(F32)
    pair = jnp.where(s_iota == slot0, gates_ref[:, 0:1], 0.0) + jnp.where(
        s_iota == slot1, gates_ref[:, 1:2], 0.0)
    high = pair.astype(BF)
    low = (pair - high.astype(F32)).astype(BF)

    @pl.loop(1, n_ep)
    def _(s):
        ret_arrival(lax.rem(me_e + s, n_ep)).wait_recv()

    back = ret[...]
    combined = dot(high, back) + dot(low, back)

    sum1 = jnp.sum(combined, axis=1, keepdims=True)
    sum2 = jnp.sum(combined * combined, axis=1, keepdims=True)
    stat[me_x] = jnp.where(lane == 0, sum1, jnp.where(lane == 1, sum2, 0.0)).T[:8]

    def stat_copy(x):
        here = stat.at[me_x]
        return pltpu.make_async_remote_copy(
            here, here, ss_sem.at[x], sr_sem.at[me_x], device_id={"tp": x})

    def stat_arrival(x):
        here = stat.at[x]
        return pltpu.make_async_remote_copy(
            here, here, ss_sem.at[x], sr_sem.at[x], device_id={"tp": x})

    @pl.loop(1, n_tp)
    def _(s):
        stat_copy(x_at(s)).start()

    @pl.loop(1, n_tp)
    def _(s):
        stat_arrival(x_at(s)).wait_recv()

    total = stat[0]
    for j in range(1, n_tp):
        total += stat[j]
    moments = jnp.concatenate([total, jnp.zeros((120, tokens), F32)], axis=0).T
    mean = moments[:, 0:1] / width
    var = moments[:, 1:2] / width - mean * mean
    out_ref[...] = (
        (combined - mean) * lax.rsqrt(var + EPS) * gain_ref[...] + bias_ref[...]
    ).astype(BF)

    @pl.loop(1, n_tp)
    def _(s):
        x = x_at(s)
        w_copy(s - 1).wait_send()
        z_copy(x, wpart).wait_send()
        stat_copy(x).wait_send()

    sib_copy().wait_send()
    ret_copy(me_y, 1 - me_c).wait_send()
    for side in range(2):
        for step in range(1, far + 1):
            hid_copy(me_y, step, side).wait_send()

    @pl.loop(1, n_y)
    def _(i):
        chip = chip_at(i)
        for core in range(CORES):
            y_copy(chip, core).wait_send()
            ret_copy(chip, core).wait_send()
        for side in range(2):
            x_copy(chip, side).wait_send()
            for step in range(1, far + 1):
                hid_copy(chip, step, side).wait_send()


def on_device(sizes, tokens, expert_ids, gates, w_gate, w_up, w_down, norm_gain, norm_bias):
    n_ep, n_tp, n_grp = sizes
    n_y = n_ep // CORES
    tok_rows, width = tokens.shape
    ff = w_gate.shape[2]
    cols = norm_gain.shape[0]
    slots = n_ep * CAP
    far = n_tp // 2
    vmem = pl.BlockSpec(memory_space=pltpu.VMEM)
    hbm = pl.BlockSpec(memory_space=pl.ANY)
    dma = pltpu.SemaphoreType.DMA
    return pl.pallas_call(
        functools.partial(kernel, n_ep, n_tp, n_grp),
        out_shape=jax.ShapeDtypeStruct((tok_rows, cols), BF),
        in_specs=[hbm, vmem, vmem, hbm, hbm, hbm, vmem, vmem],
        out_specs=vmem,
        scratch_shapes=[
            pltpu.VMEM((tok_rows, width), BF),
            pltpu.VMEM((width, ff), BF),
            pltpu.VMEM((width, ff), BF),
            pltpu.VMEM((n_tp * ff, cols), BF),
            pltpu.VMEM((4, slots, width // 4), BF),
            pltpu.VMEM((2, slots, width // 4), BF),
            pltpu.VMEM((4, CAP, width // 4), BF),
            pltpu.VMEM((n_tp, slots, ff), BF),
            pltpu.VMEM((slots, cols), BF),
            pltpu.VMEM((slots, cols), BF),
            pltpu.VMEM((8, tok_rows), F32),
            pltpu.VMEM((n_tp, 8, tok_rows), F32),
            dma((4,)),
            dma((n_ep,)), dma((n_ep,)),
            dma((2, n_y)), dma((2, n_y)),
            dma((2, far, n_y)), dma((2, far, n_y)),
            dma((n_ep,)), dma((n_ep,)),
            dma((n_tp,)), dma((n_tp,)),
            dma((n_tp,)), dma((n_tp,)),
            dma((n_tp,)), dma((n_tp,)),
        ],
        compiler_params=pltpu.CompilerParams(
            collective_id=0, has_side_effects=True, vmem_limit_bytes=60 * 2**20),
    )(
        tokens, expert_ids, gates,
        w_gate.reshape(width, ff), w_up.reshape(width, ff), w_down.reshape(ff, width),
        norm_gain.reshape(1, cols), norm_bias.reshape(1, cols),
    )


def solution(mesh):
    sizes = (mesh.shape["ep"], mesh.shape["tp"], mesh.shape["grp"])
    return jax.shard_map(
        functools.partial(on_device, sizes),
        mesh=mesh,
        in_specs=(
            P(("grp", "ep"), None),
            P(("grp", "ep"), None),
            P(("grp", "ep"), None),
            P("ep", None, "tp"),
            P("ep", None, "tp"),
            P("ep", "tp", None),
            P("tp"),
            P("tp"),
        ),
        out_specs=P(("grp", "ep"), "tp"),
        check_vma=False,
    )
```

```python
import functools

import jax
import jax.numpy as jnp
from jax import lax
from jax.experimental import pallas as pl
from jax.experimental.pallas import tpu as pltpu
from jax.sharding import PartitionSpec as P

CAP = 64
CORES = 2
EPS = 1e-05
BF = jnp.bfloat16
F32 = jnp.float32


def dot(a, b):
    return jnp.dot(a, b, preferred_element_type=F32)


FAR = 4
QUARTER_TYPE, THREE_TYPE, FULL_TYPE = 3, 5, 7
PLAN = (
    ("B", 0), ("A", 1), ("W", 0), ("C1", 0), ("A2", 1), ("W", 1),
    ("A", 2), ("A", 3), ("C2", 0), ("B", 1), ("A2", 2), ("A2", 3),
    ("C3", 0), ("C1", 1), ("B", 2), ("B", 3), ("D", 0), ("C2", 1),
    ("C1", 2), ("C1", 3), ("C3", 1), ("C2", 2), ("C2", 3), ("A", 4),
    ("A", 5), ("D", 1), ("C3", 2), ("C3", 3), ("B", 4), ("B", 5),
    ("D", 2), ("C1", 4), ("D", 3), ("C1", 5), ("C2", 4), ("C2", 5),
    ("C3", 4), ("C3", 5), ("D", 4), ("B", 6), ("B", 7), ("D", 5),
    ("C1", 6), ("C1", 7), ("C2", 6), ("C2", 7), ("C3", 6), ("C3", 7),
    ("D", 6), ("D", 7),
)
STAGES = ("A", "A2", "B", "C1", "C2", "C3", "D", "W")


def offset_of(i):
    size = FAR - i // 2
    return jnp.where(i == 0, 0, size * (2 * lax.rem(i, 2) - 1))


def near_offset(i):
    return (i // 2 + 1) * (1 - 2 * lax.rem(i, 2))


def kernel(
    n_ep, n_tp, n_grp,
    tok_hbm, ids_ref, gates_ref, wg_hbm, wu_hbm, wd_hbm, gain_ref, bias_ref,
    out_ref,
    tok, wg, wu, wdc, routed, sendb, sib, hid, outb, ret, slots, stat, high, low,
    load_sem,
    ys_sem, yr_sem, xs_sem, xr_sem, hs_sem, hr_sem, rs_sem, rr_sem,
    ws_sem, wr_sem, zs_sem, zr_sem, ss_sem, sr_sem,
):
    n_y = n_ep // CORES
    tokens, width = tok.shape
    quarter = width // 4
    cols = width // n_tp
    ff = wg.shape[1]
    rows = CORES * CAP
    far = n_tp // 2
    me_g, me_e, me_x = (lax.axis_index(a) for a in ("grp", "ep", "tp"))
    me_y, me_c = me_e // CORES, lax.rem(me_e, CORES)
    kind = lax.rem(me_x, 4)
    side_cols = (slice(0, quarter // 2), slice(quarter // 2, quarter))
    right, left = lax.rem(me_x + 1, n_tp), lax.rem(me_x + n_tp - 1, n_tp)
    mate = me_g + 1 - 2 * lax.rem(me_g, 2)
    wpart = lax.rem(me_g, 2)

    def x_at(s):
        return lax.rem(me_x + s + n_tp, n_tp)

    def chip_at(i):
        return lax.rem(me_y + offset_of(i) + n_y, n_y)

    def chunk_rows(chip):
        return pl.ds(pl.multiple_of(chip * rows, rows), rows)

    def block_rows(block):
        return pl.ds(pl.multiple_of(block * CAP, CAP), CAP)

    load_tok = pltpu.make_async_copy(tok_hbm, tok, load_sem.at[0])
    load_wg = pltpu.make_async_copy(wg_hbm, wg, load_sem.at[1])
    load_wu = pltpu.make_async_copy(wu_hbm, wu, load_sem.at[2])
    own_cols = pl.ds(pl.multiple_of(me_x * cols, cols), cols)
    own_w = pl.ds(pl.multiple_of(me_x * ff, ff), ff)
    load_wd = pltpu.make_async_copy(wd_hbm.at[:, own_cols], wdc.at[own_w], load_sem.at[3])
    load_tok.start()
    load_wg.start()
    load_wu.start()
    load_wd.start()

    barrier = pltpu.get_barrier_semaphore()
    for s in range(1, n_ep):
        pl.semaphore_signal(barrier, 1, device_id={"ep": lax.rem(me_e + s, n_ep)})
    for s in range(1, n_tp):
        pl.semaphore_signal(barrier, 1, device_id={"tp": lax.rem(me_x + s, n_tp)})
    pl.semaphore_signal(barrier, 1, device_id={"grp": mate})

    lane = lax.broadcasted_iota(jnp.int32, (tokens, 128), 1)
    columns = jnp.concatenate(
        [ids_ref[...].astype(F32), gates_ref[...], jnp.zeros((124, tokens), F32)], axis=0).T
    lane_f = lane.astype(F32)
    hit0 = lane_f == columns[:, 0:1]
    hit1 = lane_f == columns[:, 1:2]
    named = jnp.where(hit0 | hit1, 1.0, 0.0).astype(BF)
    t_row = lax.broadcasted_iota(jnp.int32, (tokens, tokens), 0)
    t_col = lax.broadcasted_iota(jnp.int32, (tokens, tokens), 1)
    before = jnp.where(t_col < t_row, 1.0, 0.0).astype(BF)
    position = dot(before, named)
    slot = position + (lane * CAP).astype(F32)
    slot0 = jnp.sum(jnp.where(hit0, slot, 0.0), axis=1, keepdims=True)
    slot1 = jnp.sum(jnp.where(hit1, slot, 0.0), axis=1, keepdims=True)
    slots[...] = jnp.where(lane == 0, slot0, jnp.where(lane == 1, slot1, -1.0)).T[:8]

    pl.semaphore_wait(barrier, n_ep - 1 + n_tp - 1 + 1)

    wrows = ff // 2

    def w_half(x, part):
        return pl.ds(pl.multiple_of(x * ff + part * wrows, wrows), wrows)

    def w_copy(i):
        x = x_at(near_offset(i))
        return pltpu.make_async_remote_copy(
            wd_hbm.at[
                pl.ds(pl.multiple_of(wpart * wrows, wrows), wrows),
                pl.ds(pl.multiple_of(x * cols, cols), cols),
            ],
            wdc.at[w_half(me_x, wpart)],
            ws_sem.at[x], wr_sem.at[me_x], device_id={"tp": x},
        )

    def w_arrival(x):
        here = wdc.at[w_half(x, wpart)]
        return pltpu.make_async_remote_copy(
            here, here, ws_sem.at[x], wr_sem.at[x], device_id={"tp": x})

    def z_copy(x, part):
        here = wdc.at[w_half(x, part)]
        return pltpu.make_async_remote_copy(
            here, here, zs_sem.at[x], zr_sem.at[x], device_id={"grp": mate})

    @pl.loop(0, n_tp - 1)
    def _(i):
        w_copy(i).start()

    load_tok.wait()

    def spread(chip, column):
        s_iota = (chip * rows).astype(F32) + lax.broadcasted_iota(
            jnp.int32, (rows, tokens), 0).astype(F32)
        chosen = (s_iota == slots[0:1, :]) | (s_iota == slots[1:2, :])
        pick = jnp.where(chosen, 1.0, 0.0).astype(BF)
        return dot(pick, tok[:, pl.ds(pl.multiple_of(column, quarter), quarter)]).astype(BF)

    def quarter_of(k):
        return lax.rem(kind + k, 4)

    def y_copy(chip, core, q):
        expert = chip * CORES + core
        return pltpu.make_async_remote_copy(
            sendb.at[q, block_rows(expert)],
            routed.at[q, block_rows(me_e)],
            ys_sem.at[q, expert], yr_sem.at[q, me_e], device_id={"ep": expert},
        )

    def y_arrival(block, q):
        here = routed.at[q, block_rows(block)]
        return pltpu.make_async_remote_copy(
            here, here, ys_sem.at[q, block], yr_sem.at[q, block], device_id={"ep": block})

    def sent_quarters(i):
        first = jnp.where((i > QUARTER_TYPE) & (i <= THREE_TYPE), 1, 0)
        return first, jnp.where(i <= QUARTER_TYPE, 1, 4)

    sibling = me_y * CORES + 1 - me_c

    def sib_copy():
        return pltpu.make_async_remote_copy(
            sib, routed.at[:, block_rows(me_e)],
            ys_sem.at[0, sibling], yr_sem.at[0, me_e], device_id={"ep": sibling},
        )

    def sib_arrival():
        here = routed.at[:, block_rows(sibling)]
        return pltpu.make_async_remote_copy(
            here, here, ys_sem.at[0, sibling], yr_sem.at[0, sibling], device_id={"ep": sibling})

    @pl.loop(1, n_y)
    def _(i):
        chip = chip_at(i)

        def send(k, carry):
            q = quarter_of(k)
            sendb[q, chunk_rows(chip), :] = spread(chip, q * quarter)
            for core in range(CORES):
                y_copy(chip, core, q).start()
            return carry

        lax.fori_loop(*sent_quarters(i), send, 0)

    @pl.loop(0, 4)
    def _(q):
        both = spread(me_y, q * quarter)
        swap = me_c == 0
        routed[q, block_rows(me_e), :] = jnp.where(swap, both[:CAP], both[CAP:])
        sib[q] = jnp.where(swap, both[CAP:], both[:CAP])

    sib_copy().start()

    s_iota = lax.broadcasted_iota(jnp.int32, (tokens, n_ep * CAP), 1).astype(F32)
    pair = jnp.where(s_iota == slot0, columns[:, 2:3], 0.0) + jnp.where(
        s_iota == slot1, columns[:, 3:4], 0.0)
    high[...] = pair.astype(BF)
    low[...] = (pair - high[...].astype(F32)).astype(BF)

    def x_move(part, side, step, chip, arriving):
        peer = ((right, left), (left, right))[arriving][side]
        return pltpu.make_async_remote_copy(
            part, part, xs_sem.at[side, step, chip], xr_sem.at[side, step, chip],
            device_id={"tp": peer})

    def whole(k, chip):
        return routed.at[quarter_of(k), chunk_rows(chip)]

    def half_of(k, chip, side):
        return routed.at[quarter_of(k), chunk_rows(chip), side_cols[side]]

    def x_copy_q(chip, side):
        return x_move(whole(0, chip), side, 0, chip, False)

    def x_arrival_q(chip, side):
        return x_move(whole((3, 1)[side], chip), side, 0, chip, True)

    def x_copy_q2(chip, side):
        return x_move(half_of((3, 1)[side], chip, side), side, 1, chip, False)

    def x_arrival_q2(chip, side):
        return x_move(half_of(2, chip, side), side, 1, chip, True)

    def x_copy_t(chip, side):
        return x_move(half_of((1, 3)[side], chip, side), side, 0, chip, False)

    def x_arrival_t(chip, side):
        return x_move(half_of(0, chip, side), side, 0, chip, True)

    def hid_part(chip, x, step, side):
        if step < far:
            return hid.at[x, chunk_rows(chip)]
        first = pl.multiple_of(chip * rows + side * CAP, CAP)
        return hid.at[x, pl.ds(first, rows // 2)]

    def hid_copy(chip, step, side):
        x = x_at((1 - step, step - 1)[side])
        here = hid_part(chip, x, step, side)
        return pltpu.make_async_remote_copy(
            here, here, hs_sem.at[side, step - 1, chip], hr_sem.at[side, step - 1, chip],
            device_id={"tp": (right, left)[side]})

    def hid_arrival(chip, step, side):
        x = x_at((-step, step)[side])
        here = hid_part(chip, x, step, side)
        return pltpu.make_async_remote_copy(
            here, here, hs_sem.at[side, step - 1, chip], hr_sem.at[side, step - 1, chip],
            device_id={"tp": (left, right)[side]})

    def ret_copy(chip, core):
        block = chip * CORES + core
        return pltpu.make_async_remote_copy(
            outb.at[block_rows(block)], ret.at[block_rows(me_e)],
            rs_sem.at[block], rr_sem.at[me_e], device_id={"ep": block})

    def ret_arrival(expert):
        here = ret.at[block_rows(expert)]
        return pltpu.make_async_remote_copy(
            here, here, rs_sem.at[expert], rr_sem.at[expert], device_id={"ep": expert})

    def y_wait(i, chip):
        def one(k, carry):
            for core in range(CORES):
                y_arrival(chip * CORES + core, quarter_of(k)).wait_recv()
            return carry

        lax.fori_loop(*sent_quarters(i), one, 0)

    def first_layers(chip):
        here = chunk_rows(chip)
        gate = jnp.zeros((rows, ff), F32)
        up = jnp.zeros((rows, ff), F32)
        for q in range(4):
            part = routed[q, here, :]
            at = slice(q * quarter, (q + 1) * quarter)
            gate += dot(part, wg[at, :])
            up += dot(part, wu[at, :])
        hid[me_x, here, :] = (gate / (1.0 + jnp.exp(-gate)) * up).astype(BF)
        for side in range(2):
            hid_copy(chip, 1, side).start()

    def relay(chip, step):
        for side in range(2):
            hid_arrival(chip, step, side).wait_recv()
            hid_copy(chip, step + 1, side).start()

    def last_layer(chip):
        for side in range(2):
            hid_arrival(chip, far, side).wait_recv()
        here = chunk_rows(chip)
        acc = jnp.zeros((rows, cols), F32)
        for j in range(n_tp):
            acc += dot(hid[j, here, :], wdc[j * ff:(j + 1) * ff, :])
        outb[here, :] = acc.astype(BF)

    def at_event(e):
        code = jnp.int32(0)
        for n, (stage, i) in enumerate(PLAN):
            code = jnp.where(e == n, STAGES.index(stage) * n_y + i, code)
        return code // n_y, lax.rem(code, n_y)

    @pl.loop(0, len(PLAN))
    def _(e):
        stage, i = at_event(e)
        chip = chip_at(i)

        def when(name):
            return pl.when(stage == STAGES.index(name))

        @when("A")
        def _():
            y_wait(i, chip)

            @pl.when(i <= QUARTER_TYPE)
            def _():
                for side in range(2):
                    x_copy_q(chip, side).start()

            @pl.when(i > QUARTER_TYPE)
            def _():
                for side in range(2):
                    x_copy_t(chip, side).start()

        @when("A2")
        def _():
            for side in range(2):
                x_arrival_q(chip, side).wait_recv()
                x_copy_q2(chip, side).start()

        @when("B")
        def _():
            @pl.when(i == 0)
            def _():
                sib_arrival().wait_recv()
                load_wg.wait()
                load_wu.wait()

            @pl.when((i > 0) & (i <= QUARTER_TYPE))
            def _():
                for side in range(2):
                    x_arrival_q2(chip, side).wait_recv()

            @pl.when((i > QUARTER_TYPE) & (i <= THREE_TYPE))
            def _():
                for side in range(2):
                    x_arrival_t(chip, side).wait_recv()

            @pl.when(i > THREE_TYPE)
            def _():
                y_wait(i, chip)

            first_layers(chip)

        for step in range(1, far):
            @when(f"C{step}")
            def _():
                relay(chip, step)

        @when("W")
        def _():
            for n in range(n_tp // 2):
                @pl.when((i == 0) == (n < n_tp // 4))
                def _():
                    for s in sorted({n + 1, -n - 1 + n_tp}):
                        x = x_at(s)
                        w_arrival(x).wait_recv()
                        z_copy(x, wpart).start()

        @when("D")
        def _():
            @pl.when(i == 0)
            def _():
                @pl.loop(1, n_tp)
                def _(s):
                    z_copy(x_at(s), 1 - wpart).wait_recv()
                load_wd.wait()

            last_layer(chip)

            @pl.when(i == 0)
            def _():
                ret[block_rows(me_e), :] = outb[block_rows(me_e), :]
                ret_copy(me_y, 1 - me_c).start()

            @pl.when(i > 0)
            def _():
                for core in range(CORES):
                    ret_copy(chip, core).start()

    @pl.loop(1, n_ep)
    def _(s):
        ret_arrival(lax.rem(me_e + s, n_ep)).wait_recv()

    back = ret[...]
    combined = dot(high[...], back) + dot(low[...], back)

    sum1 = jnp.sum(combined, axis=1, keepdims=True)
    sum2 = jnp.sum(combined * combined, axis=1, keepdims=True)
    stat[me_x] = jnp.where(lane == 0, sum1, jnp.where(lane == 1, sum2, 0.0)).T[:8]

    def stat_copy(x):
        here = stat.at[me_x]
        return pltpu.make_async_remote_copy(
            here, here, ss_sem.at[x], sr_sem.at[me_x], device_id={"tp": x})

    def stat_arrival(x):
        here = stat.at[x]
        return pltpu.make_async_remote_copy(
            here, here, ss_sem.at[x], sr_sem.at[x], device_id={"tp": x})

    @pl.loop(1, n_tp)
    def _(s):
        stat_copy(x_at(s)).start()

    @pl.loop(1, n_tp)
    def _(s):
        stat_arrival(x_at(s)).wait_recv()

    total = stat[0]
    for j in range(1, n_tp):
        total += stat[j]
    moments = jnp.concatenate([total, jnp.zeros((120, tokens), F32)], axis=0).T
    mean = moments[:, 0:1] / width
    var = moments[:, 1:2] / width - mean * mean
    out_ref[...] = (
        (combined - mean) * lax.rsqrt(var + EPS) * gain_ref[...] + bias_ref[...]
    ).astype(BF)

    @pl.loop(1, n_tp)
    def _(s):
        x = x_at(s)
        w_copy(s - 1).wait_send()
        z_copy(x, wpart).wait_send()
        stat_copy(x).wait_send()

    sib_copy().wait_send()
    ret_copy(me_y, 1 - me_c).wait_send()
    for side in range(2):
        for step in range(1, far + 1):
            hid_copy(me_y, step, side).wait_send()

    @pl.loop(1, n_y)
    def _(i):
        chip = chip_at(i)

        def gone(k, carry):
            for core in range(CORES):
                y_copy(chip, core, quarter_of(k)).wait_send()
            return carry

        lax.fori_loop(*sent_quarters(i), gone, 0)
        for core in range(CORES):
            ret_copy(chip, core).wait_send()

        @pl.when(i <= QUARTER_TYPE)
        def _():
            for side in range(2):
                x_copy_q(chip, side).wait_send()
                x_copy_q2(chip, side).wait_send()

        @pl.when((i > QUARTER_TYPE) & (i <= THREE_TYPE))
        def _():
            for side in range(2):
                x_copy_t(chip, side).wait_send()

        for side in range(2):
            for step in range(1, far + 1):
                hid_copy(chip, step, side).wait_send()


def on_device(sizes, tokens, expert_ids, gates, w_gate, w_up, w_down, norm_gain, norm_bias):
    n_ep, n_tp, n_grp = sizes
    n_y = n_ep // CORES
    tok_rows, width = tokens.shape
    ff = w_gate.shape[2]
    cols = norm_gain.shape[0]
    slots = n_ep * CAP
    far = n_tp // 2
    vmem = pl.BlockSpec(memory_space=pltpu.VMEM)
    hbm = pl.BlockSpec(memory_space=pl.ANY)
    dma = pltpu.SemaphoreType.DMA
    return pl.pallas_call(
        functools.partial(kernel, n_ep, n_tp, n_grp),
        out_shape=jax.ShapeDtypeStruct((tok_rows, cols), BF),
        in_specs=[hbm, vmem, vmem, hbm, hbm, hbm, vmem, vmem],
        out_specs=vmem,
        scratch_shapes=[
            pltpu.VMEM((tok_rows, width), BF),
            pltpu.VMEM((width, ff), BF),
            pltpu.VMEM((width, ff), BF),
            pltpu.VMEM((n_tp * ff, cols), BF),
            pltpu.VMEM((4, slots, width // 4), BF),
            pltpu.VMEM((4, slots, width // 4), BF),
            pltpu.VMEM((4, CAP, width // 4), BF),
            pltpu.VMEM((n_tp, slots, ff), BF),
            pltpu.VMEM((slots, cols), BF),
            pltpu.VMEM((slots, cols), BF),
            pltpu.VMEM((8, tok_rows), F32),
            pltpu.VMEM((n_tp, 8, tok_rows), F32),
            pltpu.VMEM((tok_rows, slots), BF),
            pltpu.VMEM((tok_rows, slots), BF),
            dma((4,)),
            dma((4, n_ep)), dma((4, n_ep)),
            dma((2, 2, n_y)), dma((2, 2, n_y)),
            dma((2, far, n_y)), dma((2, far, n_y)),
            dma((n_ep,)), dma((n_ep,)),
            dma((n_tp,)), dma((n_tp,)),
            dma((n_tp,)), dma((n_tp,)),
            dma((n_tp,)), dma((n_tp,)),
        ],
        compiler_params=pltpu.CompilerParams(
            collective_id=0, has_side_effects=True, vmem_limit_bytes=60 * 2**20),
    )(
        tokens, expert_ids.T, gates.T,
        w_gate.reshape(width, ff), w_up.reshape(width, ff), w_down.reshape(ff, width),
        norm_gain.reshape(1, cols), norm_bias.reshape(1, cols),
    )


def solution(mesh):
    sizes = (mesh.shape["ep"], mesh.shape["tp"], mesh.shape["grp"])
    return jax.shard_map(
        functools.partial(on_device, sizes),
        mesh=mesh,
        in_specs=(
            P(("grp", "ep"), None),
            P(("grp", "ep"), None),
            P(("grp", "ep"), None),
            P("ep", None, "tp"),
            P("ep", None, "tp"),
            P("ep", "tp", None),
            P("tp"),
            P("tp"),
        ),
        out_specs=P(("grp", "ep"), "tp"),
        check_vma=False,
    )
```

```python
import functools

import jax
import jax.numpy as jnp
from jax import lax
from jax.experimental import pallas as pl
from jax.experimental.pallas import tpu as pltpu
from jax.sharding import PartitionSpec as P

CAP = 64
CORES = 2
EPS = 1e-05
BF = jnp.bfloat16
F32 = jnp.float32


def dot(a, b):
    return jnp.dot(a, b, preferred_element_type=F32)


OFFSETS = (0, 3, -3, 4, 2, -2, 1, -1)
QUARTERS = {0: (0, 4, 1), 1: (0, 4, 1), 2: (0, 2, 2), 3: (0, 1, 1), 4: (0, 1, 1)}
STAGES = ("S", "W", "O", "G", "Y", "A", "A2", "B", "C1", "C2", "C3", "D")
PLAN = (
    ("S", 2), ("S", 3), ("S", 1), ("Y", 2), ("Y", 1), ("S", 0),
    ("Y", 3), ("G", 0), ("A", 2), ("Y", 5), ("O", 0), ("Y", 7),
    ("W", 0), ("Y", 4), ("A", 1), ("A2", 2), ("W", 1), ("A", 3),
    ("A2", 1), ("A2", 3), ("B", 2), ("B", 0), ("B", 1), ("Y", 6),
    ("C1", 2), ("B", 3), ("A", 4), ("C1", 1), ("A", 5), ("C1", 3),
    ("C2", 1), ("C2", 2), ("B", 4), ("B", 5), ("C2", 3), ("C3", 1),
    ("C3", 2), ("B", 6), ("C3", 3), ("C1", 4), ("C1", 5), ("B", 7),
    ("D", 1), ("D", 2), ("C1", 0), ("C2", 5), ("C2", 4), ("C1", 6),
    ("C1", 7), ("D", 3), ("C3", 4), ("C3", 5), ("C2", 6), ("C2", 7),
    ("D", 4), ("C2", 0), ("D", 5), ("C3", 6), ("C3", 7), ("D", 6),
    ("C3", 0), ("D", 7), ("D", 0),
)
FIRST_B, FIRST_D = 2, 1
RETURNS = (2, 1, 3, 5, 4, 7, 6, 0)


def among(i, values):
    out = jnp.int32(values[0])
    for n, value in enumerate(values[1:], 1):
        out = jnp.where(i == n, value, out)
    return out


def offset_of(i):
    return among(i, OFFSETS)


def near_offset(i):
    return (i // 2 + 1) * (1 - 2 * lax.rem(i, 2))


def kernel(
    n_ep, n_tp, n_grp,
    tok_hbm, ids_ref, gates_ref, wg_hbm, wu_hbm, wd_hbm, gain_ref, bias_ref,
    out_ref,
    tok, wg, wu, wdc, routed, sendb, sib, hid, outb, ret, slots, stat, high, low, mixed,
    load_sem,
    ys_sem, yr_sem, xs_sem, xr_sem, hs_sem, hr_sem, rs_sem, rr_sem,
    ws_sem, wr_sem, zs_sem, zr_sem, ss_sem, sr_sem,
):
    n_y = n_ep // CORES
    tokens, width = tok.shape
    quarter = width // 4
    cols = width // n_tp
    ff = wg.shape[1]
    rows = CORES * CAP
    far = n_tp // 2
    me_g, me_e, me_x = (lax.axis_index(a) for a in ("grp", "ep", "tp"))
    me_y, me_c = me_e // CORES, lax.rem(me_e, CORES)
    kind = lax.rem(me_x, 4)
    side_cols = (slice(0, quarter // 2), slice(quarter // 2, quarter))
    right, left = lax.rem(me_x + 1, n_tp), lax.rem(me_x + n_tp - 1, n_tp)
    mate = me_g + 1 - 2 * lax.rem(me_g, 2)
    wpart = lax.rem(me_g, 2)

    def x_at(s):
        return lax.rem(me_x + s + n_tp, n_tp)

    def chip_at(i):
        return lax.rem(me_y + offset_of(i) + n_y, n_y)

    def chunk_rows(chip):
        return pl.ds(pl.multiple_of(chip * rows, rows), rows)

    def block_rows(block):
        return pl.ds(pl.multiple_of(block * CAP, CAP), CAP)

    load_tok = pltpu.make_async_copy(tok_hbm, tok, load_sem.at[0])
    load_wg = pltpu.make_async_copy(wg_hbm, wg, load_sem.at[1])
    load_wu = pltpu.make_async_copy(wu_hbm, wu, load_sem.at[2])
    own_cols = pl.ds(pl.multiple_of(me_x * cols, cols), cols)
    own_w = pl.ds(pl.multiple_of(me_x * ff, ff), ff)
    load_wd = pltpu.make_async_copy(wd_hbm.at[:, own_cols], wdc.at[own_w], load_sem.at[3])
    barrier = pltpu.get_barrier_semaphore()
    for s in range(1, n_ep):
        pl.semaphore_signal(barrier, 1, device_id={"ep": lax.rem(me_e + s, n_ep)})
    for s in range(1, n_tp):
        pl.semaphore_signal(barrier, 1, device_id={"tp": lax.rem(me_x + s, n_tp)})
    pl.semaphore_signal(barrier, 1, device_id={"grp": mate})

    load_tok.start()
    load_wg.start()
    load_wu.start()
    load_wd.start()

    lane = lax.broadcasted_iota(jnp.int32, (tokens, 128), 1)
    columns = jnp.concatenate(
        [ids_ref[...].astype(F32), gates_ref[...], jnp.zeros((124, tokens), F32)], axis=0).T
    lane_f = lane.astype(F32)
    hit0 = lane_f == columns[:, 0:1]
    hit1 = lane_f == columns[:, 1:2]
    named = jnp.where(hit0 | hit1, 1.0, 0.0).astype(BF)
    t_row = lax.broadcasted_iota(jnp.int32, (tokens, tokens), 0)
    t_col = lax.broadcasted_iota(jnp.int32, (tokens, tokens), 1)
    before = jnp.where(t_col < t_row, 1.0, 0.0).astype(BF)
    position = dot(before, named)
    slot = position + (lane * CAP).astype(F32)
    slot0 = jnp.sum(jnp.where(hit0, slot, 0.0), axis=1, keepdims=True)
    slot1 = jnp.sum(jnp.where(hit1, slot, 0.0), axis=1, keepdims=True)
    slots[...] = jnp.where(lane == 0, slot0, jnp.where(lane == 1, slot1, -1.0)).T[:8]

    pl.semaphore_wait(barrier, n_ep - 1 + n_tp - 1 + 1)

    wrows = ff // 2

    def w_half(x, part):
        return pl.ds(pl.multiple_of(x * ff + part * wrows, wrows), wrows)

    def w_copy(i):
        x = x_at(near_offset(i))
        return pltpu.make_async_remote_copy(
            wd_hbm.at[
                pl.ds(pl.multiple_of(wpart * wrows, wrows), wrows),
                pl.ds(pl.multiple_of(x * cols, cols), cols),
            ],
            wdc.at[w_half(me_x, wpart)],
            ws_sem.at[x], wr_sem.at[me_x], device_id={"tp": x},
        )

    def w_arrival(x):
        here = wdc.at[w_half(x, wpart)]
        return pltpu.make_async_remote_copy(
            here, here, ws_sem.at[x], wr_sem.at[x], device_id={"tp": x})

    def z_copy(x, part):
        here = wdc.at[w_half(x, part)]
        return pltpu.make_async_remote_copy(
            here, here, zs_sem.at[x], zr_sem.at[x], device_id={"grp": mate})


    def spread(chip, column):
        s_iota = (chip * rows).astype(F32) + lax.broadcasted_iota(
            jnp.int32, (rows, tokens), 0).astype(F32)
        chosen = (s_iota == slots[0:1, :]) | (s_iota == slots[1:2, :])
        pick = jnp.where(chosen, 1.0, 0.0).astype(BF)
        return dot(pick, tok[:, pl.ds(pl.multiple_of(column, quarter), quarter)]).astype(BF)

    def quarter_of(k):
        return lax.rem(kind + k, 4)

    def y_copy(chip, core, q):
        expert = chip * CORES + core
        return pltpu.make_async_remote_copy(
            sendb.at[q, block_rows(expert)],
            routed.at[q, block_rows(me_e)],
            ys_sem.at[q, expert], yr_sem.at[q, me_e], device_id={"ep": expert},
        )

    def y_arrival(block, q):
        here = routed.at[q, block_rows(block)]
        return pltpu.make_async_remote_copy(
            here, here, ys_sem.at[q, block], yr_sem.at[q, block], device_id={"ep": block})

    def each_quarter(i, act):
        spec = [QUARTERS[abs(d)] for d in OFFSETS]
        first, number, stride = (among(i, [q[n] for q in spec]) for n in range(3))

        def one(k, carry):
            act(quarter_of(first + k * stride))
            return carry

        lax.fori_loop(0, number, one, 0)

    sibling = me_y * CORES + 1 - me_c

    def sib_copy():
        return pltpu.make_async_remote_copy(
            sib, routed.at[:, block_rows(me_e)],
            ys_sem.at[0, sibling], yr_sem.at[0, me_e], device_id={"ep": sibling},
        )

    def sib_arrival():
        here = routed.at[:, block_rows(sibling)]
        return pltpu.make_async_remote_copy(
            here, here, ys_sem.at[0, sibling], yr_sem.at[0, sibling], device_id={"ep": sibling})

    def dispatch(i, chip):
        def send(q):
            sendb[q, chunk_rows(chip), :] = spread(chip, q * quarter)
            for core in range(CORES):
                y_copy(chip, core, q).start()

        each_quarter(i, send)

    def own_rows():
        @pl.loop(0, 4)
        def _(q):
            both = spread(me_y, q * quarter)
            swap = me_c == 0
            routed[q, block_rows(me_e), :] = jnp.where(swap, both[:CAP], both[CAP:])
            sib[q] = jnp.where(swap, both[CAP:], both[:CAP])

        sib_copy().start()

    def x_move(part, side, step, chip, arriving):
        peer = ((right, left), (left, right))[arriving][side]
        return pltpu.make_async_remote_copy(
            part, part, xs_sem.at[side, step, chip], xr_sem.at[side, step, chip],
            device_id={"tp": peer})

    def whole(k, chip):
        return routed.at[quarter_of(k), chunk_rows(chip)]

    def half_of(k, chip, side):
        return routed.at[quarter_of(k), chunk_rows(chip), side_cols[side]]

    def x_copy_q(chip, side):
        return x_move(whole(0, chip), side, 0, chip, False)

    def x_arrival_q(chip, side):
        return x_move(whole((3, 1)[side], chip), side, 0, chip, True)

    def x_copy_q2(chip, side):
        return x_move(half_of((3, 1)[side], chip, side), side, 1, chip, False)

    def x_arrival_q2(chip, side):
        return x_move(half_of(2, chip, side), side, 1, chip, True)

    def hid_part(chip, x, step, side):
        if step < far:
            return hid.at[x, chunk_rows(chip)]
        first = pl.multiple_of(chip * rows + side * CAP, CAP)
        return hid.at[x, pl.ds(first, rows // 2)]

    def hid_copy(chip, step, side):
        x = x_at((1 - step, step - 1)[side])
        here = hid_part(chip, x, step, side)
        return pltpu.make_async_remote_copy(
            here, here, hs_sem.at[side, step - 1, chip], hr_sem.at[side, step - 1, chip],
            device_id={"tp": (right, left)[side]})

    def hid_arrival(chip, step, side):
        x = x_at((-step, step)[side])
        here = hid_part(chip, x, step, side)
        return pltpu.make_async_remote_copy(
            here, here, hs_sem.at[side, step - 1, chip], hr_sem.at[side, step - 1, chip],
            device_id={"tp": (left, right)[side]})

    def ret_copy(chip, core):
        block = chip * CORES + core
        return pltpu.make_async_remote_copy(
            outb.at[block_rows(block)], ret.at[block_rows(me_e)],
            rs_sem.at[block], rr_sem.at[me_e], device_id={"ep": block})

    def ret_arrival(expert):
        here = ret.at[block_rows(expert)]
        return pltpu.make_async_remote_copy(
            here, here, rs_sem.at[expert], rr_sem.at[expert], device_id={"ep": expert})

    def y_wait(i, chip):
        def arrived(q):
            for core in range(CORES):
                y_arrival(chip * CORES + core, q).wait_recv()

        each_quarter(i, arrived)

    def first_layers(chip):
        here = chunk_rows(chip)
        gate = jnp.zeros((rows, ff), F32)
        up = jnp.zeros((rows, ff), F32)
        for q in range(4):
            part = routed[q, here, :]
            at = slice(q * quarter, (q + 1) * quarter)
            gate += dot(part, wg[at, :])
            up += dot(part, wu[at, :])
        hid[me_x, here, :] = (gate / (1.0 + jnp.exp(-gate)) * up).astype(BF)
        for side in range(2):
            hid_copy(chip, 1, side).start()

    def relay(chip, step):
        for side in range(2):
            hid_arrival(chip, step, side).wait_recv()
            hid_copy(chip, step + 1, side).start()

    def last_layer(chip):
        for side in range(2):
            hid_arrival(chip, far, side).wait_recv()
        here = chunk_rows(chip)
        acc = jnp.zeros((rows, cols), F32)
        for j in range(n_tp):
            acc += dot(hid[j, here, :], wdc[j * ff:(j + 1) * ff, :])
        outb[here, :] = acc.astype(BF)

    def pair_weights():
        s_iota = lax.broadcasted_iota(jnp.int32, (tokens, n_ep * CAP), 1).astype(F32)
        pair = jnp.where(s_iota == slot0, columns[:, 2:3], 0.0) + jnp.where(
            s_iota == slot1, columns[:, 3:4], 0.0)
        high[...] = pair.astype(BF)
        low[...] = (pair - high[...].astype(F32)).astype(BF)

    def is_sent(i, number):
        return among(i, [QUARTERS[abs(d)][1] for d in OFFSETS]) == number

    load_tok.wait()

    @pl.loop(0, len(PLAN))
    def _(e):
        code = among(e, [STAGES.index(stage) * n_y + i for stage, i in PLAN])
        stage, i = code // n_y, lax.rem(code, n_y)
        chip = chip_at(i)

        def when(name):
            return pl.when(stage == STAGES.index(name))

        @when("S")
        def _():
            w_copy(2 * i).start()

            @pl.when(i < n_tp // 2 - 1)
            def _():
                w_copy(2 * i + 1).start()

        @when("W")
        def _():
            for n in range(n_tp // 2):
                @pl.when((i == 0) == (n < n_tp // 4))
                def _():
                    for s in sorted({n + 1, -n - 1 + n_tp}):
                        x = x_at(s)
                        w_arrival(x).wait_recv()
                        z_copy(x, wpart).start()

        @when("O")
        def _():
            own_rows()

        @when("G")
        def _():
            pair_weights()

        @when("Y")
        def _():
            dispatch(i, chip)

        @when("A")
        def _():
            y_wait(i, chip)
            for side in range(2):
                x_copy_q(chip, side).start()

        @when("A2")
        def _():
            for side in range(2):
                x_arrival_q(chip, side).wait_recv()
                x_copy_q2(chip, side).start()

        @when("B")
        def _():
            @pl.when(i == FIRST_B)
            def _():
                load_wg.wait()
                load_wu.wait()

            @pl.when(i == 0)
            def _():
                sib_arrival().wait_recv()

            @pl.when((i > 0) & is_sent(i, 1))
            def _():
                for side in range(2):
                    x_arrival_q2(chip, side).wait_recv()

            @pl.when((i > 0) & is_sent(i, 2))
            def _():
                for side in range(2):
                    x_arrival_q(chip, side).wait_recv()

            @pl.when((i > 0) & is_sent(i, 4))
            def _():
                y_wait(i, chip)

            first_layers(chip)

        for step in range(1, far):
            @when(f"C{step}")
            def _():
                relay(chip, step)

        @when("D")
        def _():
            @pl.when(i == FIRST_D)
            def _():
                @pl.loop(1, n_tp)
                def _(s):
                    z_copy(x_at(s), 1 - wpart).wait_recv()
                load_wd.wait()

            last_layer(chip)

            @pl.when(i == 0)
            def _():
                ret[block_rows(me_e), :] = outb[block_rows(me_e), :]
                ret_copy(me_y, 1 - me_c).start()

            @pl.when(i > 0)
            def _():
                for core in range(CORES):
                    ret_copy(chip, core).start()

    mixed[...] = jnp.zeros_like(mixed)

    @pl.loop(0, n_y)
    def _(n):
        i = among(n, RETURNS)
        chip = chip_at(i)

        @pl.when(i == 0)
        def _():
            ret_arrival(sibling).wait_recv()

        @pl.when(i > 0)
        def _():
            for core in range(CORES):
                ret_arrival(chip * CORES + core).wait_recv()

        back = ret[chunk_rows(chip), :]
        at = chunk_rows(chip)
        mixed[...] += dot(high[:, at], back) + dot(low[:, at], back)

    combined = mixed[...]

    sum1 = jnp.sum(combined, axis=1, keepdims=True)
    sum2 = jnp.sum(combined * combined, axis=1, keepdims=True)
    stat[me_x] = jnp.where(lane == 0, sum1, jnp.where(lane == 1, sum2, 0.0)).T[:8]

    def stat_copy(x):
        here = stat.at[me_x]
        return pltpu.make_async_remote_copy(
            here, here, ss_sem.at[x], sr_sem.at[me_x], device_id={"tp": x})

    def stat_arrival(x):
        here = stat.at[x]
        return pltpu.make_async_remote_copy(
            here, here, ss_sem.at[x], sr_sem.at[x], device_id={"tp": x})

    @pl.loop(1, n_tp)
    def _(s):
        stat_copy(x_at(s)).start()

    @pl.loop(1, n_tp)
    def _(s):
        w_copy(s - 1).wait_send()
        z_copy(x_at(s), wpart).wait_send()

    sib_copy().wait_send()
    ret_copy(me_y, 1 - me_c).wait_send()
    for side in range(2):
        for step in range(1, far + 1):
            hid_copy(me_y, step, side).wait_send()

    @pl.loop(1, n_y)
    def _(i):
        chip = chip_at(i)
        for core in range(CORES):
            ret_copy(chip, core).wait_send()

        def gone(q):
            for core in range(CORES):
                y_copy(chip, core, q).wait_send()

        each_quarter(i, gone)

        for side in range(2):
            @pl.when(jnp.logical_not(is_sent(i, 4)))
            def _():
                x_copy_q(chip, side).wait_send()

            @pl.when(is_sent(i, 1))
            def _():
                x_copy_q2(chip, side).wait_send()

            for step in range(1, far + 1):
                hid_copy(chip, step, side).wait_send()

    @pl.loop(1, n_tp)
    def _(s):
        stat_arrival(x_at(s)).wait_recv()
        stat_copy(x_at(s)).wait_send()

    total = stat[0]
    for j in range(1, n_tp):
        total += stat[j]
    moments = jnp.concatenate([total, jnp.zeros((120, tokens), F32)], axis=0).T
    mean = moments[:, 0:1] / width
    var = moments[:, 1:2] / width - mean * mean
    out_ref[...] = (
        (combined - mean) * lax.rsqrt(var + EPS) * gain_ref[...] + bias_ref[...]
    ).astype(BF)


def on_device(sizes, tokens, expert_ids, gates, w_gate, w_up, w_down, norm_gain, norm_bias):
    n_ep, n_tp, n_grp = sizes
    n_y = n_ep // CORES
    tok_rows, width = tokens.shape
    ff = w_gate.shape[2]
    cols = norm_gain.shape[0]
    slots = n_ep * CAP
    far = n_tp // 2
    vmem = pl.BlockSpec(memory_space=pltpu.VMEM)
    hbm = pl.BlockSpec(memory_space=pl.ANY)
    dma = pltpu.SemaphoreType.DMA
    return pl.pallas_call(
        functools.partial(kernel, n_ep, n_tp, n_grp),
        out_shape=jax.ShapeDtypeStruct((tok_rows, cols), BF),
        in_specs=[hbm, vmem, vmem, hbm, hbm, hbm, vmem, vmem],
        out_specs=vmem,
        scratch_shapes=[
            pltpu.VMEM((tok_rows, width), BF),
            pltpu.VMEM((width, ff), BF),
            pltpu.VMEM((width, ff), BF),
            pltpu.VMEM((n_tp * ff, cols), BF),
            pltpu.VMEM((4, slots, width // 4), BF),
            pltpu.VMEM((4, slots, width // 4), BF),
            pltpu.VMEM((4, CAP, width // 4), BF),
            pltpu.VMEM((n_tp, slots, ff), BF),
            pltpu.VMEM((slots, cols), BF),
            pltpu.VMEM((slots, cols), BF),
            pltpu.VMEM((8, tok_rows), F32),
            pltpu.VMEM((n_tp, 8, tok_rows), F32),
            pltpu.VMEM((tok_rows, slots), BF),
            pltpu.VMEM((tok_rows, slots), BF),
            pltpu.VMEM((tok_rows, cols), F32),
            dma((4,)),
            dma((4, n_ep)), dma((4, n_ep)),
            dma((2, 2, n_y)), dma((2, 2, n_y)),
            dma((2, far, n_y)), dma((2, far, n_y)),
            dma((n_ep,)), dma((n_ep,)),
            dma((n_tp,)), dma((n_tp,)),
            dma((n_tp,)), dma((n_tp,)),
            dma((n_tp,)), dma((n_tp,)),
        ],
        compiler_params=pltpu.CompilerParams(
            collective_id=0, has_side_effects=True, vmem_limit_bytes=60 * 2**20),
    )(
        tokens, expert_ids.T, gates.T,
        w_gate.reshape(width, ff), w_up.reshape(width, ff), w_down.reshape(ff, width),
        norm_gain.reshape(1, cols), norm_bias.reshape(1, cols),
    )


def solution(mesh):
    sizes = (mesh.shape["ep"], mesh.shape["tp"], mesh.shape["grp"])
    return jax.shard_map(
        functools.partial(on_device, sizes),
        mesh=mesh,
        in_specs=(
            P(("grp", "ep"), None),
            P(("grp", "ep"), None),
            P(("grp", "ep"), None),
            P("ep", None, "tp"),
            P("ep", None, "tp"),
            P("ep", "tp", None),
            P("tp"),
            P("tp"),
        ),
        out_specs=P(("grp", "ep"), "tp"),
        check_vma=False,
    )
```

```python
import functools

import jax
import jax.numpy as jnp
from jax import lax
from jax.experimental import pallas as pl
from jax.experimental.pallas import tpu as pltpu
from jax.sharding import PartitionSpec as P

CAP = 64
CORES = 2
EPS = 1e-05
BF = jnp.bfloat16
F32 = jnp.float32


def dot(a, b):
    return jnp.dot(a, b, preferred_element_type=F32)


OFFSETS = (0, 3, -3, 4, 2, -2, 1, -1)
QUARTERS = {0: (0, 4, 1), 1: (0, 4, 1), 2: (0, 2, 2), 3: (0, 1, 1), 4: (0, 1, 1)}
STAGES = ("S", "W", "O", "G", "Y", "A", "A2", "B", "C1", "C2", "C3", "D")
PLAN = (
    ("S", 0), ("Y", 2), ("S", 3), ("Y", 1), ("Y", 3), ("Y", 5),
    ("S", 2), ("Y", 4), ("Y", 6), ("O", 0), ("S", 1), ("Y", 7),
    ("G", 0), ("A", 2), ("A", 1), ("B", 0), ("A2", 2), ("A2", 1),
    ("A", 3), ("B", 2), ("W", 1), ("B", 1), ("A2", 3), ("C1", 2),
    ("C1", 1), ("A", 4), ("A", 5), ("C2", 2), ("B", 3), ("W", 0),
    ("B", 4), ("B", 5), ("C3", 2), ("C2", 1), ("C1", 3), ("C1", 4),
    ("C1", 5), ("C3", 1), ("B", 7), ("D", 2), ("C2", 3), ("B", 6),
    ("C2", 4), ("C2", 5), ("D", 1), ("C3", 3), ("C1", 6), ("C3", 4),
    ("C1", 7), ("C1", 0), ("C3", 5), ("D", 3), ("C2", 6), ("D", 4),
    ("C2", 7), ("D", 5), ("C2", 0), ("C3", 6), ("C3", 7), ("C3", 0),
    ("D", 6), ("D", 7), ("D", 0),
)
FIRST_B, FIRST_D = 0, 2
RETURNS = (1, 2, 3, 5, 4, 7, 6, 0)


def among(i, values):
    out = jnp.int32(values[0])
    for n, value in enumerate(values[1:], 1):
        out = jnp.where(i == n, value, out)
    return out


def offset_of(i):
    return among(i, OFFSETS)


def near_offset(i):
    return (i // 2 + 1) * (1 - 2 * lax.rem(i, 2))


def kernel(
    n_ep, n_tp, n_grp,
    tok_hbm, ids_ref, gates_ref, wg_hbm, wu_hbm, wd_hbm, gain_ref, bias_ref,
    out_ref,
    tok, wg, wu, wdc, routed, sendb, sib, hid, outb, ret, slots, stat, high, low, mixed,
    load_sem,
    ys_sem, yr_sem, xs_sem, xr_sem, hs_sem, hr_sem, rs_sem, rr_sem,
    ws_sem, wr_sem, zs_sem, zr_sem, ss_sem, sr_sem,
):
    n_y = n_ep // CORES
    tokens, width = tok.shape
    quarter = width // 4
    cols = width // n_tp
    ff = wg.shape[1]
    rows = CORES * CAP
    far = n_tp // 2
    me_g, me_e, me_x = (lax.axis_index(a) for a in ("grp", "ep", "tp"))
    me_y, me_c = me_e // CORES, lax.rem(me_e, CORES)
    kind = lax.rem(me_x, 4)
    side_cols = (slice(0, quarter // 2), slice(quarter // 2, quarter))
    right, left = lax.rem(me_x + 1, n_tp), lax.rem(me_x + n_tp - 1, n_tp)
    mate = me_g + 1 - 2 * lax.rem(me_g, 2)
    wpart = lax.rem(me_g, 2)

    def x_at(s):
        return lax.rem(me_x + s + n_tp, n_tp)

    def chip_at(i):
        return lax.rem(me_y + offset_of(i) + n_y, n_y)

    def chunk_rows(chip):
        return pl.ds(pl.multiple_of(chip * rows, rows), rows)

    def block_rows(block):
        return pl.ds(pl.multiple_of(block * CAP, CAP), CAP)

    load_tok = pltpu.make_async_copy(tok_hbm, tok, load_sem.at[0])
    load_wg = pltpu.make_async_copy(wg_hbm, wg, load_sem.at[1])
    load_wu = pltpu.make_async_copy(wu_hbm, wu, load_sem.at[2])
    own_cols = pl.ds(pl.multiple_of(me_x * cols, cols), cols)
    own_w = pl.ds(pl.multiple_of(me_x * ff, ff), ff)
    load_wd = pltpu.make_async_copy(wd_hbm.at[:, own_cols], wdc.at[own_w], load_sem.at[3])
    barrier = pltpu.get_barrier_semaphore()
    for s in range(1, n_ep):
        pl.semaphore_signal(barrier, 1, device_id={"ep": lax.rem(me_e + s, n_ep)})
    for s in range(1, n_tp):
        pl.semaphore_signal(barrier, 1, device_id={"tp": lax.rem(me_x + s, n_tp)})
    pl.semaphore_signal(barrier, 1, device_id={"grp": mate})

    load_tok.start()
    load_wg.start()
    load_wu.start()
    load_wd.start()

    lane = lax.broadcasted_iota(jnp.int32, (tokens, 128), 1)
    columns = jnp.concatenate(
        [ids_ref[...].astype(F32), gates_ref[...], jnp.zeros((124, tokens), F32)], axis=0).T
    lane_f = lane.astype(F32)
    hit0 = lane_f == columns[:, 0:1]
    hit1 = lane_f == columns[:, 1:2]
    named = jnp.where(hit0 | hit1, 1.0, 0.0).astype(BF)
    t_row = lax.broadcasted_iota(jnp.int32, (tokens, tokens), 0)
    t_col = lax.broadcasted_iota(jnp.int32, (tokens, tokens), 1)
    before = jnp.where(t_col < t_row, 1.0, 0.0).astype(BF)
    position = dot(before, named)
    slot = position + (lane * CAP).astype(F32)
    slot0 = jnp.sum(jnp.where(hit0, slot, 0.0), axis=1, keepdims=True)
    slot1 = jnp.sum(jnp.where(hit1, slot, 0.0), axis=1, keepdims=True)
    slots[...] = jnp.where(lane == 0, slot0, jnp.where(lane == 1, slot1, -1.0)).T[:8]

    pl.semaphore_wait(barrier, n_ep - 1 + n_tp - 1 + 1)

    wrows = ff // 2

    def w_half(x, part):
        return pl.ds(pl.multiple_of(x * ff + part * wrows, wrows), wrows)

    def w_copy(i):
        x = x_at(near_offset(i))
        return pltpu.make_async_remote_copy(
            wd_hbm.at[
                pl.ds(pl.multiple_of(wpart * wrows, wrows), wrows),
                pl.ds(pl.multiple_of(x * cols, cols), cols),
            ],
            wdc.at[w_half(me_x, wpart)],
            ws_sem.at[x], wr_sem.at[me_x], device_id={"tp": x},
        )

    def w_arrival(x):
        here = wdc.at[w_half(x, wpart)]
        return pltpu.make_async_remote_copy(
            here, here, ws_sem.at[x], wr_sem.at[x], device_id={"tp": x})

    def z_copy(x, part):
        here = wdc.at[w_half(x, part)]
        return pltpu.make_async_remote_copy(
            here, here, zs_sem.at[x], zr_sem.at[x], device_id={"grp": mate})


    def spread(chip, column):
        s_iota = (chip * rows).astype(F32) + lax.broadcasted_iota(
            jnp.int32, (rows, tokens), 0).astype(F32)
        chosen = (s_iota == slots[0:1, :]) | (s_iota == slots[1:2, :])
        pick = jnp.where(chosen, 1.0, 0.0).astype(BF)
        return dot(pick, tok[:, pl.ds(pl.multiple_of(column, quarter), quarter)]).astype(BF)

    def quarter_of(k):
        return lax.rem(kind + k, 4)

    def y_copy(chip, core, q):
        expert = chip * CORES + core
        return pltpu.make_async_remote_copy(
            sendb.at[q, block_rows(expert)],
            routed.at[q, block_rows(me_e)],
            ys_sem.at[q, expert], yr_sem.at[q, me_e], device_id={"ep": expert},
        )

    def y_arrival(block, q):
        here = routed.at[q, block_rows(block)]
        return pltpu.make_async_remote_copy(
            here, here, ys_sem.at[q, block], yr_sem.at[q, block], device_id={"ep": block})

    def each_quarter(i, act):
        spec = [QUARTERS[abs(d)] for d in OFFSETS]
        first, number, stride = (among(i, [q[n] for q in spec]) for n in range(3))

        def one(k, carry):
            act(quarter_of(first + k * stride))
            return carry

        lax.fori_loop(0, number, one, 0)

    sibling = me_y * CORES + 1 - me_c

    def sib_copy():
        return pltpu.make_async_remote_copy(
            sib, routed.at[:, block_rows(me_e)],
            ys_sem.at[0, sibling], yr_sem.at[0, me_e], device_id={"ep": sibling},
        )

    def sib_arrival():
        here = routed.at[:, block_rows(sibling)]
        return pltpu.make_async_remote_copy(
            here, here, ys_sem.at[0, sibling], yr_sem.at[0, sibling], device_id={"ep": sibling})

    def dispatch(i, chip):
        def send(q):
            sendb[q, chunk_rows(chip), :] = spread(chip, q * quarter)
            for core in range(CORES):
                y_copy(chip, core, q).start()

        each_quarter(i, send)

    def own_rows():
        @pl.loop(0, 4)
        def _(q):
            both = spread(me_y, q * quarter)
            swap = me_c == 0
            routed[q, block_rows(me_e), :] = jnp.where(swap, both[:CAP], both[CAP:])
            sib[q] = jnp.where(swap, both[CAP:], both[:CAP])

        sib_copy().start()

    def x_move(part, side, step, chip, arriving):
        peer = ((right, left), (left, right))[arriving][side]
        return pltpu.make_async_remote_copy(
            part, part, xs_sem.at[side, step, chip], xr_sem.at[side, step, chip],
            device_id={"tp": peer})

    def whole(k, chip):
        return routed.at[quarter_of(k), chunk_rows(chip)]

    def half_of(k, chip, side):
        return routed.at[quarter_of(k), chunk_rows(chip), side_cols[side]]

    def x_copy_q(chip, side):
        return x_move(whole(0, chip), side, 0, chip, False)

    def x_arrival_q(chip, side):
        return x_move(whole((3, 1)[side], chip), side, 0, chip, True)

    def x_copy_q2(chip, side):
        return x_move(half_of((3, 1)[side], chip, side), side, 1, chip, False)

    def x_arrival_q2(chip, side):
        return x_move(half_of(2, chip, side), side, 1, chip, True)

    def hid_part(chip, x, step, side):
        if step < far:
            return hid.at[x, chunk_rows(chip)]
        first = pl.multiple_of(chip * rows + side * CAP, CAP)
        return hid.at[x, pl.ds(first, rows // 2)]

    def hid_copy(chip, step, side):
        x = x_at((1 - step, step - 1)[side])
        here = hid_part(chip, x, step, side)
        return pltpu.make_async_remote_copy(
            here, here, hs_sem.at[side, step - 1, chip], hr_sem.at[side, step - 1, chip],
            device_id={"tp": (right, left)[side]})

    def hid_arrival(chip, step, side):
        x = x_at((-step, step)[side])
        here = hid_part(chip, x, step, side)
        return pltpu.make_async_remote_copy(
            here, here, hs_sem.at[side, step - 1, chip], hr_sem.at[side, step - 1, chip],
            device_id={"tp": (left, right)[side]})

    def ret_copy(chip, core):
        block = chip * CORES + core
        return pltpu.make_async_remote_copy(
            outb.at[block_rows(block)], ret.at[block_rows(me_e)],
            rs_sem.at[block], rr_sem.at[me_e], device_id={"ep": block})

    def ret_arrival(expert):
        here = ret.at[block_rows(expert)]
        return pltpu.make_async_remote_copy(
            here, here, rs_sem.at[expert], rr_sem.at[expert], device_id={"ep": expert})

    def y_wait(i, chip):
        def arrived(q):
            for core in range(CORES):
                y_arrival(chip * CORES + core, q).wait_recv()

        each_quarter(i, arrived)

    def first_layers(chip):
        here = chunk_rows(chip)
        gate = jnp.zeros((rows, ff), F32)
        up = jnp.zeros((rows, ff), F32)
        for q in range(4):
            part = routed[q, here, :]
            at = slice(q * quarter, (q + 1) * quarter)
            gate += dot(part, wg[at, :])
            up += dot(part, wu[at, :])
        hid[me_x, here, :] = (gate / (1.0 + jnp.exp(-gate)) * up).astype(BF)
        for side in range(2):
            hid_copy(chip, 1, side).start()

    def relay(chip, step):
        for side in range(2):
            hid_arrival(chip, step, side).wait_recv()
            hid_copy(chip, step + 1, side).start()

    def last_layer(chip):
        for side in range(2):
            hid_arrival(chip, far, side).wait_recv()
        here = chunk_rows(chip)
        acc = jnp.zeros((rows, cols), F32)
        for j in range(n_tp):
            acc += dot(hid[j, here, :], wdc[j * ff:(j + 1) * ff, :])
        outb[here, :] = acc.astype(BF)

    def pair_weights():
        s_iota = lax.broadcasted_iota(jnp.int32, (tokens, n_ep * CAP), 1).astype(F32)
        pair = jnp.where(s_iota == slot0, columns[:, 2:3], 0.0) + jnp.where(
            s_iota == slot1, columns[:, 3:4], 0.0)
        high[...] = pair.astype(BF)
        low[...] = (pair - high[...].astype(F32)).astype(BF)

    def is_sent(i, number):
        return among(i, [QUARTERS[abs(d)][1] for d in OFFSETS]) == number

    load_tok.wait()

    @pl.loop(0, len(PLAN))
    def _(e):
        code = among(e, [STAGES.index(stage) * n_y + i for stage, i in PLAN])
        stage, i = code // n_y, lax.rem(code, n_y)
        chip = chip_at(i)

        def when(name):
            return pl.when(stage == STAGES.index(name))

        @when("S")
        def _():
            w_copy(2 * i).start()

            @pl.when(i < n_tp // 2 - 1)
            def _():
                w_copy(2 * i + 1).start()

        @when("W")
        def _():
            for n in range(n_tp // 2):
                @pl.when((i == 0) == (n < n_tp // 4))
                def _():
                    for s in sorted({n + 1, -n - 1 + n_tp}):
                        x = x_at(s)
                        w_arrival(x).wait_recv()
                        z_copy(x, wpart).start()

        @when("O")
        def _():
            own_rows()

        @when("G")
        def _():
            pair_weights()

        @when("Y")
        def _():
            dispatch(i, chip)

        @when("A")
        def _():
            y_wait(i, chip)
            for side in range(2):
                x_copy_q(chip, side).start()

        @when("A2")
        def _():
            for side in range(2):
                x_arrival_q(chip, side).wait_recv()
                x_copy_q2(chip, side).start()

        @when("B")
        def _():
            @pl.when(i == FIRST_B)
            def _():
                load_wg.wait()
                load_wu.wait()

            @pl.when(i == 0)
            def _():
                sib_arrival().wait_recv()

            @pl.when((i > 0) & is_sent(i, 1))
            def _():
                for side in range(2):
                    x_arrival_q2(chip, side).wait_recv()

            @pl.when((i > 0) & is_sent(i, 2))
            def _():
                for side in range(2):
                    x_arrival_q(chip, side).wait_recv()

            @pl.when((i > 0) & is_sent(i, 4))
            def _():
                y_wait(i, chip)

            first_layers(chip)

        for step in range(1, far):
            @when(f"C{step}")
            def _():
                relay(chip, step)

        @when("D")
        def _():
            @pl.when(i == FIRST_D)
            def _():
                @pl.loop(1, n_tp)
                def _(s):
                    z_copy(x_at(s), 1 - wpart).wait_recv()
                load_wd.wait()

            last_layer(chip)

            @pl.when(i == 0)
            def _():
                ret[block_rows(me_e), :] = outb[block_rows(me_e), :]
                ret_copy(me_y, 1 - me_c).start()

            @pl.when(i > 0)
            def _():
                for core in range(CORES):
                    ret_copy(chip, core).start()

    mixed[...] = jnp.zeros_like(mixed)

    @pl.loop(0, n_y)
    def _(n):
        i = among(n, RETURNS)
        chip = chip_at(i)

        @pl.when(i == 0)
        def _():
            ret_arrival(sibling).wait_recv()

        @pl.when(i > 0)
        def _():
            for core in range(CORES):
                ret_arrival(chip * CORES + core).wait_recv()

        back = ret[chunk_rows(chip), :]
        at = chunk_rows(chip)
        mixed[...] += dot(high[:, at], back) + dot(low[:, at], back)

    combined = mixed[...]

    sum1 = jnp.sum(combined, axis=1, keepdims=True)
    sum2 = jnp.sum(combined * combined, axis=1, keepdims=True)
    stat[me_x] = jnp.where(lane == 0, sum1, jnp.where(lane == 1, sum2, 0.0)).T[:8]

    def stat_copy(x):
        here = stat.at[me_x]
        return pltpu.make_async_remote_copy(
            here, here, ss_sem.at[x], sr_sem.at[me_x], device_id={"tp": x})

    def stat_arrival(x):
        here = stat.at[x]
        return pltpu.make_async_remote_copy(
            here, here, ss_sem.at[x], sr_sem.at[x], device_id={"tp": x})

    @pl.loop(1, n_tp)
    def _(s):
        stat_copy(x_at(s)).start()

    @pl.loop(1, n_tp)
    def _(s):
        w_copy(s - 1).wait_send()
        z_copy(x_at(s), wpart).wait_send()

    sib_copy().wait_send()
    ret_copy(me_y, 1 - me_c).wait_send()
    for side in range(2):
        for step in range(1, far + 1):
            hid_copy(me_y, step, side).wait_send()

    @pl.loop(1, n_y)
    def _(i):
        chip = chip_at(i)
        for core in range(CORES):
            ret_copy(chip, core).wait_send()

        def gone(q):
            for core in range(CORES):
                y_copy(chip, core, q).wait_send()

        each_quarter(i, gone)

        for side in range(2):
            @pl.when(jnp.logical_not(is_sent(i, 4)))
            def _():
                x_copy_q(chip, side).wait_send()

            @pl.when(is_sent(i, 1))
            def _():
                x_copy_q2(chip, side).wait_send()

            for step in range(1, far + 1):
                hid_copy(chip, step, side).wait_send()

    @pl.loop(1, n_tp)
    def _(s):
        stat_arrival(x_at(s)).wait_recv()
        stat_copy(x_at(s)).wait_send()

    total = stat[0]
    for j in range(1, n_tp):
        total += stat[j]
    moments = jnp.concatenate([total, jnp.zeros((120, tokens), F32)], axis=0).T
    mean = moments[:, 0:1] / width
    var = moments[:, 1:2] / width - mean * mean
    out_ref[...] = (
        (combined - mean) * lax.rsqrt(var + EPS) * gain_ref[...] + bias_ref[...]
    ).astype(BF)


def on_device(sizes, tokens, expert_ids, gates, w_gate, w_up, w_down, norm_gain, norm_bias):
    n_ep, n_tp, n_grp = sizes
    n_y = n_ep // CORES
    tok_rows, width = tokens.shape
    ff = w_gate.shape[2]
    cols = norm_gain.shape[0]
    slots = n_ep * CAP
    far = n_tp // 2
    vmem = pl.BlockSpec(memory_space=pltpu.VMEM)
    hbm = pl.BlockSpec(memory_space=pl.ANY)
    dma = pltpu.SemaphoreType.DMA
    return pl.pallas_call(
        functools.partial(kernel, n_ep, n_tp, n_grp),
        out_shape=jax.ShapeDtypeStruct((tok_rows, cols), BF),
        in_specs=[hbm, vmem, vmem, hbm, hbm, hbm, vmem, vmem],
        out_specs=vmem,
        scratch_shapes=[
            pltpu.VMEM((tok_rows, width), BF),
            pltpu.VMEM((width, ff), BF),
            pltpu.VMEM((width, ff), BF),
            pltpu.VMEM((n_tp * ff, cols), BF),
            pltpu.VMEM((4, slots, width // 4), BF),
            pltpu.VMEM((4, slots, width // 4), BF),
            pltpu.VMEM((4, CAP, width // 4), BF),
            pltpu.VMEM((n_tp, slots, ff), BF),
            pltpu.VMEM((slots, cols), BF),
            pltpu.VMEM((slots, cols), BF),
            pltpu.VMEM((8, tok_rows), F32),
            pltpu.VMEM((n_tp, 8, tok_rows), F32),
            pltpu.VMEM((tok_rows, slots), BF),
            pltpu.VMEM((tok_rows, slots), BF),
            pltpu.VMEM((tok_rows, cols), F32),
            dma((4,)),
            dma((4, n_ep)), dma((4, n_ep)),
            dma((2, 2, n_y)), dma((2, 2, n_y)),
            dma((2, far, n_y)), dma((2, far, n_y)),
            dma((n_ep,)), dma((n_ep,)),
            dma((n_tp,)), dma((n_tp,)),
            dma((n_tp,)), dma((n_tp,)),
            dma((n_tp,)), dma((n_tp,)),
        ],
        compiler_params=pltpu.CompilerParams(
            collective_id=0, has_side_effects=True, vmem_limit_bytes=60 * 2**20),
    )(
        tokens, expert_ids.T, gates.T,
        w_gate.reshape(width, ff), w_up.reshape(width, ff), w_down.reshape(ff, width),
        norm_gain.reshape(1, cols), norm_bias.reshape(1, cols),
    )


def solution(mesh):
    sizes = (mesh.shape["ep"], mesh.shape["tp"], mesh.shape["grp"])
    return jax.shard_map(
        functools.partial(on_device, sizes),
        mesh=mesh,
        in_specs=(
            P(("grp", "ep"), None),
            P(("grp", "ep"), None),
            P(("grp", "ep"), None),
            P("ep", None, "tp"),
            P("ep", None, "tp"),
            P("ep", "tp", None),
            P("tp"),
            P("tp"),
        ),
        out_specs=P(("grp", "ep"), "tp"),
        check_vma=False,
    )
```

```python
import functools

import jax
import jax.numpy as jnp
from jax import lax
from jax.experimental import pallas as pl
from jax.experimental.pallas import tpu as pltpu
from jax.sharding import PartitionSpec as P

CAP = 64
CORES = 2
EPS = 1e-05
BF = jnp.bfloat16
F32 = jnp.float32


def dot(a, b):
    return jnp.dot(a, b, preferred_element_type=F32)


OFFSETS = (0, 3, -3, 4, 2, -2, 1, -1)
QUARTERS = {0: (0, 4, 1), 1: (0, 4, 1), 2: (0, 2, 2), 3: (0, 1, 1), 4: (0, 1, 1)}
STAGES = ("S", "W", "O", "G", "Y", "A", "A2", "B", "C1", "C2", "C3", "D")
PLAN = (
    ("S", 0), ("Y", 2), ("S", 3), ("Y", 1), ("Y", 3), ("Y", 5),
    ("S", 2), ("Y", 4), ("Y", 6), ("O", 0), ("S", 1), ("Y", 7),
    ("G", 0), ("A", 2), ("A", 1), ("B", 0), ("A2", 2), ("A2", 1),
    ("A", 3), ("B", 2), ("W", 1), ("B", 1), ("A2", 3), ("C1", 2),
    ("C1", 1), ("A", 4), ("A", 5), ("C2", 2), ("B", 3), ("W", 0),
    ("B", 4), ("B", 5), ("C3", 2), ("C2", 1), ("C1", 3), ("C1", 4),
    ("C1", 5), ("C3", 1), ("B", 7), ("D", 2), ("C2", 3), ("B", 6),
    ("C2", 4), ("C2", 5), ("D", 1), ("C3", 3), ("C1", 6), ("C3", 4),
    ("C1", 7), ("C1", 0), ("C3", 5), ("D", 3), ("C2", 6), ("D", 4),
    ("C2", 7), ("D", 5), ("C2", 0), ("C3", 6), ("C3", 7), ("C3", 0),
    ("D", 6), ("D", 7), ("D", 0),
)
FIRST_B, FIRST_D = 0, 2
RETURNS = (1, 2, 3, 5, 4, 7, 6, 0)


def among(i, values):
    out = jnp.int32(values[0])
    for n, value in enumerate(values[1:], 1):
        out = jnp.where(i == n, value, out)
    return out


def offset_of(i):
    return among(i, OFFSETS)


def near_offset(i):
    return (i // 2 + 1) * (1 - 2 * lax.rem(i, 2))


def kernel(
    n_ep, n_tp, n_grp,
    tok_hbm, ids_ref, gates_ref, wg_hbm, wu_hbm, wd_hbm, gain_ref, bias_ref,
    out_ref,
    tok, wg, wu, wdc, routed, sendb, sib, hid, outb, ret, slots, stat, high, low, mixed,
    load_sem,
    ys_sem, yr_sem, xs_sem, xr_sem, hs_sem, hr_sem, rs_sem, rr_sem,
    ws_sem, wr_sem, zs_sem, zr_sem, ss_sem, sr_sem,
):
    n_y = n_ep // CORES
    tokens, width = tok.shape
    quarter = width // 4
    cols = width // n_tp
    ff = wg.shape[1]
    rows = CORES * CAP
    far = n_tp // 2
    me_g, me_e, me_x = (lax.axis_index(a) for a in ("grp", "ep", "tp"))
    me_y, me_c = me_e // CORES, lax.rem(me_e, CORES)
    kind = lax.rem(me_x, 4)
    side_cols = (slice(0, quarter // 2), slice(quarter // 2, quarter))
    right, left = lax.rem(me_x + 1, n_tp), lax.rem(me_x + n_tp - 1, n_tp)
    mate = me_g + 1 - 2 * lax.rem(me_g, 2)
    wpart = lax.rem(me_g, 2)

    def x_at(s):
        return lax.rem(me_x + s + n_tp, n_tp)

    def chip_at(i):
        return lax.rem(me_y + offset_of(i) + n_y, n_y)

    def chunk_rows(chip):
        return pl.ds(pl.multiple_of(chip * rows, rows), rows)

    def block_rows(block):
        return pl.ds(pl.multiple_of(block * CAP, CAP), CAP)

    load_tok = pltpu.make_async_copy(tok_hbm, tok, load_sem.at[0])
    load_wg = pltpu.make_async_copy(wg_hbm, wg, load_sem.at[1])
    load_wu = pltpu.make_async_copy(wu_hbm, wu, load_sem.at[2])
    own_cols = pl.ds(pl.multiple_of(me_x * cols, cols), cols)
    own_w = pl.ds(pl.multiple_of(me_x * ff, ff), ff)
    load_wd = pltpu.make_async_copy(wd_hbm.at[:, own_cols], wdc.at[own_w], load_sem.at[3])
    barrier = pltpu.get_barrier_semaphore()
    for s in range(1, n_ep):
        pl.semaphore_signal(barrier, 1, device_id={"ep": lax.rem(me_e + s, n_ep)})
    for s in range(1, n_tp):
        pl.semaphore_signal(barrier, 1, device_id={"tp": lax.rem(me_x + s, n_tp)})
    pl.semaphore_signal(barrier, 1, device_id={"grp": mate})

    load_tok.start()
    load_wg.start()
    load_wu.start()
    load_wd.start()

    lane = lax.broadcasted_iota(jnp.int32, (tokens, 128), 1)
    columns = jnp.concatenate(
        [ids_ref[...].astype(F32), gates_ref[...], jnp.zeros((124, tokens), F32)], axis=0).T
    lane_f = lane.astype(F32)
    hit0 = lane_f == columns[:, 0:1]
    hit1 = lane_f == columns[:, 1:2]
    named = jnp.where(hit0 | hit1, 1.0, 0.0).astype(BF)
    t_row = lax.broadcasted_iota(jnp.int32, (tokens, tokens), 0)
    t_col = lax.broadcasted_iota(jnp.int32, (tokens, tokens), 1)
    before = jnp.where(t_col < t_row, 1.0, 0.0).astype(BF)
    position = dot(before, named)
    slot = position + (lane * CAP).astype(F32)
    slot0 = jnp.sum(jnp.where(hit0, slot, 0.0), axis=1, keepdims=True)
    slot1 = jnp.sum(jnp.where(hit1, slot, 0.0), axis=1, keepdims=True)
    slots[...] = jnp.where(lane == 0, slot0, jnp.where(lane == 1, slot1, -1.0)).T[:8]

    pl.semaphore_wait(barrier, n_ep - 1 + n_tp - 1 + 1)

    wrows = ff // 2

    def w_half(x, part):
        return pl.ds(pl.multiple_of(x * ff + part * wrows, wrows), wrows)

    def w_copy(i):
        x = x_at(near_offset(i))
        return pltpu.make_async_remote_copy(
            wd_hbm.at[
                pl.ds(pl.multiple_of(wpart * wrows, wrows), wrows),
                pl.ds(pl.multiple_of(x * cols, cols), cols),
            ],
            wdc.at[w_half(me_x, wpart)],
            ws_sem.at[x], wr_sem.at[me_x], device_id={"tp": x},
        )

    def w_arrival(x):
        here = wdc.at[w_half(x, wpart)]
        return pltpu.make_async_remote_copy(
            here, here, ws_sem.at[x], wr_sem.at[x], device_id={"tp": x})

    def z_copy(x, part):
        here = wdc.at[w_half(x, part)]
        return pltpu.make_async_remote_copy(
            here, here, zs_sem.at[x], zr_sem.at[x], device_id={"grp": mate})


    def spread(chip, column):
        s_iota = (chip * rows).astype(F32) + lax.broadcasted_iota(
            jnp.int32, (rows, tokens), 0).astype(F32)
        chosen = (s_iota == slots[0:1, :]) | (s_iota == slots[1:2, :])
        pick = jnp.where(chosen, 1.0, 0.0).astype(BF)
        return dot(pick, tok[:, pl.ds(pl.multiple_of(column, quarter), quarter)]).astype(BF)

    def quarter_of(k):
        return lax.rem(kind + k, 4)

    def y_copy(chip, core, q):
        expert = chip * CORES + core
        return pltpu.make_async_remote_copy(
            sendb.at[q, block_rows(expert)],
            routed.at[q, block_rows(me_e)],
            ys_sem.at[q, expert], yr_sem.at[q, me_e], device_id={"ep": expert},
        )

    def y_arrival(block, q):
        here = routed.at[q, block_rows(block)]
        return pltpu.make_async_remote_copy(
            here, here, ys_sem.at[q, block], yr_sem.at[q, block], device_id={"ep": block})

    def each_quarter(i, act):
        spec = [QUARTERS[abs(d)] for d in OFFSETS]
        first, number, stride = (among(i, [q[n] for q in spec]) for n in range(3))

        def one(k, carry):
            act(quarter_of(first + k * stride))
            return carry

        lax.fori_loop(0, number, one, 0)

    sibling = me_y * CORES + 1 - me_c

    def sib_copy():
        return pltpu.make_async_remote_copy(
            sib, routed.at[:, block_rows(me_e)],
            ys_sem.at[0, sibling], yr_sem.at[0, me_e], device_id={"ep": sibling},
        )

    def sib_arrival():
        here = routed.at[:, block_rows(sibling)]
        return pltpu.make_async_remote_copy(
            here, here, ys_sem.at[0, sibling], yr_sem.at[0, sibling], device_id={"ep": sibling})

    def dispatch(i, chip):
        def send(q):
            sendb[q, chunk_rows(chip), :] = spread(chip, q * quarter)
            for core in range(CORES):
                y_copy(chip, core, q).start()

        each_quarter(i, send)

    def own_rows():
        @pl.loop(0, 4)
        def _(q):
            both = spread(me_y, q * quarter)
            swap = me_c == 0
            routed[q, block_rows(me_e), :] = jnp.where(swap, both[:CAP], both[CAP:])
            sib[q] = jnp.where(swap, both[CAP:], both[:CAP])

        sib_copy().start()

    def x_move(part, side, step, chip, arriving):
        peer = ((right, left), (left, right))[arriving][side]
        return pltpu.make_async_remote_copy(
            part, part, xs_sem.at[side, step, chip], xr_sem.at[side, step, chip],
            device_id={"tp": peer})

    def whole(k, chip):
        return routed.at[quarter_of(k), chunk_rows(chip)]

    def half_of(k, chip, side):
        return routed.at[quarter_of(k), chunk_rows(chip), side_cols[side]]

    def x_copy_q(chip, side):
        return x_move(whole(0, chip), side, 0, chip, False)

    def x_arrival_q(chip, side):
        return x_move(whole((3, 1)[side], chip), side, 0, chip, True)

    def x_copy_q2(chip, side):
        return x_move(half_of((3, 1)[side], chip, side), side, 1, chip, False)

    def x_arrival_q2(chip, side):
        return x_move(half_of(2, chip, side), side, 1, chip, True)

    def hid_part(chip, x, step, side):
        if step < far:
            return hid.at[x, chunk_rows(chip)]
        first = pl.multiple_of(chip * rows + side * CAP, CAP)
        return hid.at[x, pl.ds(first, rows // 2)]

    def hid_copy(chip, step, side):
        x = x_at((1 - step, step - 1)[side])
        here = hid_part(chip, x, step, side)
        return pltpu.make_async_remote_copy(
            here, here, hs_sem.at[side, step - 1, chip], hr_sem.at[side, step - 1, chip],
            device_id={"tp": (right, left)[side]})

    def hid_arrival(chip, step, side):
        x = x_at((-step, step)[side])
        here = hid_part(chip, x, step, side)
        return pltpu.make_async_remote_copy(
            here, here, hs_sem.at[side, step - 1, chip], hr_sem.at[side, step - 1, chip],
            device_id={"tp": (left, right)[side]})

    def ret_copy(chip, core):
        block = chip * CORES + core
        return pltpu.make_async_remote_copy(
            outb.at[block_rows(block)], ret.at[block_rows(me_e)],
            rs_sem.at[block], rr_sem.at[me_e], device_id={"ep": block})

    def ret_arrival(expert):
        here = ret.at[block_rows(expert)]
        return pltpu.make_async_remote_copy(
            here, here, rs_sem.at[expert], rr_sem.at[expert], device_id={"ep": expert})

    def y_wait(i, chip):
        def arrived(q):
            for core in range(CORES):
                y_arrival(chip * CORES + core, q).wait_recv()

        each_quarter(i, arrived)

    def first_layers(chip):
        here = chunk_rows(chip)
        gate = jnp.zeros((rows, ff), F32)
        up = jnp.zeros((rows, ff), F32)
        for q in range(4):
            part = routed[q, here, :]
            at = slice(q * quarter, (q + 1) * quarter)
            gate += dot(part, wg[at, :])
            up += dot(part, wu[at, :])
        hid[me_x, here, :] = (gate / (1.0 + jnp.exp(-gate)) * up).astype(BF)
        for side in range(2):
            hid_copy(chip, 1, side).start()

    def relay(chip, step):
        for side in range(2):
            hid_arrival(chip, step, side).wait_recv()
            hid_copy(chip, step + 1, side).start()

    def last_layer(chip):
        here = chunk_rows(chip)

        def term(s):
            x = x_at(s)
            at = pl.ds(pl.multiple_of(x * ff, ff), ff)
            return dot(hid[x, here, :], wdc[at, :])

        acc = term(0)
        for s in range(1, far):
            acc += term(s) + term(-s)
        for side in range(2):
            hid_arrival(chip, far, side).wait_recv()
        acc += term(far)
        outb[here, :] = acc.astype(BF)

    def pair_weights():
        s_iota = lax.broadcasted_iota(jnp.int32, (tokens, n_ep * CAP), 1).astype(F32)
        pair = jnp.where(s_iota == slot0, columns[:, 2:3], 0.0) + jnp.where(
            s_iota == slot1, columns[:, 3:4], 0.0)
        high[...] = pair.astype(BF)
        low[...] = (pair - high[...].astype(F32)).astype(BF)

    def is_sent(i, number):
        return among(i, [QUARTERS[abs(d)][1] for d in OFFSETS]) == number

    load_tok.wait()

    @pl.loop(0, len(PLAN))
    def _(e):
        code = among(e, [STAGES.index(stage) * n_y + i for stage, i in PLAN])
        stage, i = code // n_y, lax.rem(code, n_y)
        chip = chip_at(i)

        def when(name):
            return pl.when(stage == STAGES.index(name))

        @when("S")
        def _():
            w_copy(2 * i).start()

            @pl.when(i < n_tp // 2 - 1)
            def _():
                w_copy(2 * i + 1).start()

        @when("W")
        def _():
            for n in range(n_tp // 2):
                @pl.when((i == 0) == (n < n_tp // 4))
                def _():
                    for s in sorted({n + 1, -n - 1 + n_tp}):
                        x = x_at(s)
                        w_arrival(x).wait_recv()
                        z_copy(x, wpart).start()

        @when("O")
        def _():
            own_rows()

        @when("G")
        def _():
            pair_weights()

        @when("Y")
        def _():
            dispatch(i, chip)

        @when("A")
        def _():
            y_wait(i, chip)
            for side in range(2):
                x_copy_q(chip, side).start()

        @when("A2")
        def _():
            for side in range(2):
                x_arrival_q(chip, side).wait_recv()
                x_copy_q2(chip, side).start()

        @when("B")
        def _():
            @pl.when(i == FIRST_B)
            def _():
                load_wg.wait()
                load_wu.wait()

            @pl.when(i == 0)
            def _():
                sib_arrival().wait_recv()

            @pl.when((i > 0) & is_sent(i, 1))
            def _():
                for side in range(2):
                    x_arrival_q2(chip, side).wait_recv()

            @pl.when((i > 0) & is_sent(i, 2))
            def _():
                for side in range(2):
                    x_arrival_q(chip, side).wait_recv()

            @pl.when((i > 0) & is_sent(i, 4))
            def _():
                y_wait(i, chip)

            first_layers(chip)

        for step in range(1, far):
            @when(f"C{step}")
            def _():
                relay(chip, step)

        @when("D")
        def _():
            @pl.when(i == FIRST_D)
            def _():
                @pl.loop(1, n_tp)
                def _(s):
                    z_copy(x_at(s), 1 - wpart).wait_recv()
                load_wd.wait()

            last_layer(chip)

            @pl.when(i == 0)
            def _():
                ret[block_rows(me_e), :] = outb[block_rows(me_e), :]
                ret_copy(me_y, 1 - me_c).start()

            @pl.when(i > 0)
            def _():
                for core in range(CORES):
                    ret_copy(chip, core).start()

    mixed[...] = jnp.zeros_like(mixed)

    @pl.loop(0, n_y)
    def _(n):
        i = among(n, RETURNS)
        chip = chip_at(i)

        @pl.when(i == 0)
        def _():
            ret_arrival(sibling).wait_recv()

        @pl.when(i > 0)
        def _():
            for core in range(CORES):
                ret_arrival(chip * CORES + core).wait_recv()

        back = ret[chunk_rows(chip), :]
        at = chunk_rows(chip)
        mixed[...] += dot(high[:, at], back) + dot(low[:, at], back)

    combined = mixed[...]

    sum1 = jnp.sum(combined, axis=1, keepdims=True)
    sum2 = jnp.sum(combined * combined, axis=1, keepdims=True)
    stat[me_x] = jnp.where(lane == 0, sum1, jnp.where(lane == 1, sum2, 0.0)).T[:8]

    def stat_copy(x):
        here = stat.at[me_x]
        return pltpu.make_async_remote_copy(
            here, here, ss_sem.at[x], sr_sem.at[me_x], device_id={"tp": x})

    def stat_arrival(x):
        here = stat.at[x]
        return pltpu.make_async_remote_copy(
            here, here, ss_sem.at[x], sr_sem.at[x], device_id={"tp": x})

    @pl.loop(1, n_tp)
    def _(s):
        stat_copy(x_at(s)).start()

    @pl.loop(1, n_tp)
    def _(s):
        w_copy(s - 1).wait_send()
        z_copy(x_at(s), wpart).wait_send()

    sib_copy().wait_send()
    ret_copy(me_y, 1 - me_c).wait_send()
    for side in range(2):
        for step in range(1, far + 1):
            hid_copy(me_y, step, side).wait_send()

    @pl.loop(1, n_y)
    def _(i):
        chip = chip_at(i)
        for core in range(CORES):
            ret_copy(chip, core).wait_send()

        def gone(q):
            for core in range(CORES):
                y_copy(chip, core, q).wait_send()

        each_quarter(i, gone)

        for side in range(2):
            @pl.when(jnp.logical_not(is_sent(i, 4)))
            def _():
                x_copy_q(chip, side).wait_send()

            @pl.when(is_sent(i, 1))
            def _():
                x_copy_q2(chip, side).wait_send()

            for step in range(1, far + 1):
                hid_copy(chip, step, side).wait_send()

    @pl.loop(1, n_tp)
    def _(s):
        stat_arrival(x_at(s)).wait_recv()
        stat_copy(x_at(s)).wait_send()

    total = stat[0]
    for j in range(1, n_tp):
        total += stat[j]
    moments = jnp.concatenate([total, jnp.zeros((120, tokens), F32)], axis=0).T
    mean = moments[:, 0:1] / width
    var = moments[:, 1:2] / width - mean * mean
    out_ref[...] = (
        (combined - mean) * lax.rsqrt(var + EPS) * gain_ref[...] + bias_ref[...]
    ).astype(BF)


def on_device(sizes, tokens, expert_ids, gates, w_gate, w_up, w_down, norm_gain, norm_bias):
    n_ep, n_tp, n_grp = sizes
    n_y = n_ep // CORES
    tok_rows, width = tokens.shape
    ff = w_gate.shape[2]
    cols = norm_gain.shape[0]
    slots = n_ep * CAP
    far = n_tp // 2
    vmem = pl.BlockSpec(memory_space=pltpu.VMEM)
    hbm = pl.BlockSpec(memory_space=pl.ANY)
    dma = pltpu.SemaphoreType.DMA
    return pl.pallas_call(
        functools.partial(kernel, n_ep, n_tp, n_grp),
        out_shape=jax.ShapeDtypeStruct((tok_rows, cols), BF),
        in_specs=[hbm, vmem, vmem, hbm, hbm, hbm, vmem, vmem],
        out_specs=vmem,
        scratch_shapes=[
            pltpu.VMEM((tok_rows, width), BF),
            pltpu.VMEM((width, ff), BF),
            pltpu.VMEM((width, ff), BF),
            pltpu.VMEM((n_tp * ff, cols), BF),
            pltpu.VMEM((4, slots, width // 4), BF),
            pltpu.VMEM((4, slots, width // 4), BF),
            pltpu.VMEM((4, CAP, width // 4), BF),
            pltpu.VMEM((n_tp, slots, ff), BF),
            pltpu.VMEM((slots, cols), BF),
            pltpu.VMEM((slots, cols), BF),
            pltpu.VMEM((8, tok_rows), F32),
            pltpu.VMEM((n_tp, 8, tok_rows), F32),
            pltpu.VMEM((tok_rows, slots), BF),
            pltpu.VMEM((tok_rows, slots), BF),
            pltpu.VMEM((tok_rows, cols), F32),
            dma((4,)),
            dma((4, n_ep)), dma((4, n_ep)),
            dma((2, 2, n_y)), dma((2, 2, n_y)),
            dma((2, far, n_y)), dma((2, far, n_y)),
            dma((n_ep,)), dma((n_ep,)),
            dma((n_tp,)), dma((n_tp,)),
            dma((n_tp,)), dma((n_tp,)),
            dma((n_tp,)), dma((n_tp,)),
        ],
        compiler_params=pltpu.CompilerParams(
            collective_id=0, has_side_effects=True, vmem_limit_bytes=60 * 2**20),
    )(
        tokens, expert_ids.T, gates.T,
        w_gate.reshape(width, ff), w_up.reshape(width, ff), w_down.reshape(ff, width),
        norm_gain.reshape(1, cols), norm_bias.reshape(1, cols),
    )


def solution(mesh):
    sizes = (mesh.shape["ep"], mesh.shape["tp"], mesh.shape["grp"])
    return jax.shard_map(
        functools.partial(on_device, sizes),
        mesh=mesh,
        in_specs=(
            P(("grp", "ep"), None),
            P(("grp", "ep"), None),
            P(("grp", "ep"), None),
            P("ep", None, "tp"),
            P("ep", None, "tp"),
            P("ep", "tp", None),
            P("tp"),
            P("tp"),
        ),
        out_specs=P(("grp", "ep"), "tp"),
        check_vma=False,
    )
```
